512 devices in a mesh: fs: 64 (over z, y), tp: 8 (over x, core).
Axes of the slice: x: 4, y: 4, z: 16, core: 2. Of those that a mesh axis runs over, the one named last changes fastest.
Arguments:
- tokens: bfloat16 [49152, 2048], P('fs'), may hold values from -6 to 6
- norm_gain: float32 [2048], replicated, may hold values from 0.1 to 1.9
- up_weight: float32 [2048, 8192], P('fs', 'tp'), may hold values from -0.125 to 0.125
- up_scale: float32 [8192], P('tp'), may hold values from 0.5 to 2
- down_weight: float32 [8192, 2048], P('tp', 'fs'), may hold values from -0.0625 to 0.0625
- down_scale: float32 [2048], P('fs'), may hold values from 0.5 to 2
Outputs:
- output: bfloat16 [49152, 2048], P('fs', 'tp')
The draws below stay inside these ranges and needn't reach their ends.
All inputs are finite; a program needn't handle non-finite values.
Results may differ from the reference program's by a relative error of at most 0.015.
Values may be sent and summed in bfloat16 or wider, within the bound.
No kernel may reach another device: no remote copies, remote signals or barrier semaphores. Data moves between devices by JAX's collectives and lax.ppermute only.
A program may use at most 64 MiB of HBM per device.

```python
import math
import jax
import jax.numpy as jnp
from jax import lax

D = 2048
FF = 8192
TOKENS = 49152
N_TP = 8


def level_of(stream_key, dims, split, least, high):
    def one(axis_at, shards_of):
        steps = jax.random.uniform(jax.random.fold_in(jax.random.fold_in(stream_key, 6), axis_at), (shards_of,), jnp.float32, least / len(split), high / len(split))
        return jnp.repeat(jnp.exp(steps), dims[axis_at] // shards_of).reshape((-1,) + (1,) * (len(dims) - axis_at - 1))

    factor_of = one(*split[0])
    for cut in split[1:]:
        factor_of = factor_of * one(*cut)
    return factor_of


def scatter_about(rng, dims, deviation, most, pieces=(), kind=jnp.bfloat16):
    level = level_of(rng, dims, pieces, -0.22, 0.18) if pieces else 1.0
    drawn = jax.random.normal(rng, dims, jnp.float32) * deviation * level
    return jnp.minimum(jnp.maximum(drawn, -most), most).astype(kind)


def setup_inputs(seed: int = 0) -> dict:
    seeds = jax.random.split(jax.random.key(seed), 7)
    return {
        "tokens": scatter_about(seeds[0], (TOKENS, D), 1.0, 6.0, ((0, 64),)),
        "norm_gain": jnp.clip(1.0 + 0.18 * jax.random.normal(seeds[1], (D,), jnp.float32), 0.1, 1.9),
        "up_weight": scatter_about(seeds[2], (D, FF), D ** -0.5, 0.125, ((0, 64), (1, 8)), jnp.float32),
        "up_scale": jnp.clip(jnp.exp(math.log(2.0) - 1.3862944 * jax.random.uniform(seeds[3], (FF,), jnp.float32) ** level_of(seeds[3], (FF,), ((0, 8),), -0.2, 0.2)), 0.5, 2.0),
        "down_weight": scatter_about(seeds[4], (FF, D), FF ** -0.5, 0.0625, ((0, 8), (1, 64)), jnp.float32),
        "down_scale": jnp.clip(jnp.exp(math.log(2.0) - 1.3862944 * jax.random.uniform(seeds[5], (D,), jnp.float32) ** level_of(seeds[5], (D,), ((0, 64),), -0.2, 0.2)), 0.5, 2.0),
    }


epsilon = 1e-06

def reference(tokens, norm_gain, up_weight, up_scale, down_weight, down_scale):
    floats = tokens.astype(jnp.float32)
    inverse = lax.rsqrt(lax.optimization_barrier(jnp.mean(floats * floats, axis=-1, keepdims=True)) + epsilon)
    normed = (floats * inverse * norm_gain).astype(jnp.bfloat16)
    up_half = up_weight.astype(jnp.bfloat16)
    down_half = down_weight.astype(jnp.bfloat16)
    up_pre = jnp.dot(normed, up_half, preferred_element_type=jnp.float32) * up_scale
    hidden = jnp.square(jax.nn.relu(up_pre)).astype(jnp.bfloat16)
    block_width = FF // N_TP
    summed = jnp.zeros((tokens.shape[0], D), jnp.float32)
    for block in range(N_TP):
        lower = block * block_width
        partial_value = jnp.dot(hidden[:, lower:lower + block_width], down_half[lower:lower + block_width], preferred_element_type=jnp.float32).astype(jnp.bfloat16)
        summed = summed + partial_value.astype(jnp.float32)
    return (summed * down_scale).astype(jnp.bfloat16)
```

```python
import jax
import jax.numpy as jnp
from jax import lax
from jax.sharding import Mesh
from jax.sharding import PartitionSpec as P

FS = ("fs_0", "fs_1")


epsilon = 1e-06


def cut_along(array, dim, count):
    before, after = (array.shape[:dim], array.shape[dim + 1 :])
    return jnp.moveaxis(array.reshape(*before, count, -1, *after), dim, 0)


def summed_on_arrival(array, axis, dim):
    count = lax.axis_size(axis)
    tiles = lax.all_to_all(cut_along(array, dim, count), axis, 0, 0, tiled=True)
    return jnp.sum(tiles.astype(jnp.float32), axis=0)


def local(tokens, norm_gain, up_weight, up_scale, down_weight, down_scale):
    up_half = up_weight.astype(jnp.bfloat16)
    down_rows = (down_weight.T * down_scale[:, None]).astype(jnp.bfloat16)
    up_whole = lax.all_gather(up_half, FS, axis=0, tiled=True)
    down_whole = lax.all_gather(down_rows, FS, axis=0, tiled=True)
    floats = tokens.astype(jnp.float32)
    inverse = lax.rsqrt(jnp.mean(floats * floats, axis=-1, keepdims=True) + epsilon)
    normed = (floats * inverse * norm_gain).astype(jnp.bfloat16)
    up_pre = jnp.dot(normed, up_whole, preferred_element_type=jnp.float32)
    hidden = jnp.square(jax.nn.relu(up_pre * up_scale)).astype(jnp.bfloat16)
    hidden = lax.optimization_barrier(hidden)
    partial_value = lax.dot_general(
        hidden, down_whole, (((1,), (1,)), ((), ())), preferred_element_type=jnp.float32
    ).astype(jnp.bfloat16)
    return summed_on_arrival(partial_value, "tp", 1).astype(jnp.bfloat16)


def solution(mesh):
    split = Mesh(mesh.devices.reshape(16, 4, mesh.shape["tp"]), ("fs_0", "fs_1", "tp"))
    return jax.shard_map(
        local,
        mesh=split,
        in_specs=(P(FS, None), P(), P(FS, "tp"), P("tp"), P("tp", FS), P(FS)),
        out_specs=P(FS, "tp"),
        check_vma=False,
    )
```

```python
import jax
import jax.numpy as jnp
from jax import lax
from jax.experimental import pallas as pl
from jax.experimental.pallas import tpu as pltpu
from jax.sharding import Mesh
from jax.sharding import PartitionSpec as P

FS = ("z", "y")
TP = ("x", "c")

epsilon = 1e-06

LATE = 256


def spread(array, axis):
    count = lax.axis_size(axis)
    copies = jnp.broadcast_to(array[None], (count,) + array.shape)
    return lax.all_to_all(copies, axis, 0, 0, tiled=True)


def down_kernel(core_ref, hidden_ref, weight_ref, out_ref):
    groups, rows, depth = weight_ref.shape
    weight = weight_ref[...].reshape(groups * rows, depth)
    out_ref[0] = lax.dot_general(
        hidden_ref[...], weight, (((1,), (1,)), ((), ())), preferred_element_type=jnp.float32
    ).astype(out_ref.dtype)


def down_blocks(core, hidden, gathered, rows, columns, blocks, dtype):
    tokens, depth = hidden.shape
    groups = columns // rows
    return pl.pallas_call(
        down_kernel,
        grid_spec=pltpu.PrefetchScalarGridSpec(
            num_scalar_prefetch=1,
            grid=(blocks,),
            in_specs=[
                pl.BlockSpec((tokens, depth), lambda i, core_ref: (0, 0)),
                pl.BlockSpec((groups, rows, depth), lambda i, core_ref: (2 * i + core_ref[0], 0, 0)),
            ],
            out_specs=pl.BlockSpec((1, tokens, columns), lambda i, core_ref: (i, 0, 0)),
        ),
        out_shape=jax.ShapeDtypeStruct((blocks, tokens, columns), dtype),
        cost_estimate=pl.CostEstimate(
            flops=2 * tokens * depth * columns * blocks,
            bytes_accessed=2 * (tokens * depth + columns * depth * blocks + tokens * columns * blocks),
            transcendentals=0,
        ),
    )(core.reshape(1), hidden, gathered)


def local(tokens, norm_gain, up_weight, up_scale, down_weight, down_scale):
    up_half = up_weight.astype(jnp.bfloat16)
    down_rows = (down_weight.T * down_scale[:, None]).astype(jnp.bfloat16)
    rows, hidden_width = up_half.shape
    early_width = hidden_width - LATE
    parts = hidden_width // LATE
    late_rows = rows // parts
    late = jnp.concatenate(
        [up_half[i * late_rows : (i + 1) * late_rows, early_width:] for i in range(parts)], axis=1
    )
    both = spread(jnp.concatenate([down_rows, late], axis=0), "y")
    early, both = lax.optimization_barrier((up_half[:, :early_width], both))
    gathered = lax.all_gather(both, "z", axis=0, tiled=True)
    early = lax.all_gather(early, "z", axis=0, tiled=False)
    early = spread(early, "y")
    early = early.transpose(1, 0, 2, 3).reshape(-1, early_width)

    floats = tokens.astype(jnp.float32)
    inverse = lax.rsqrt(jnp.mean(floats * floats, axis=-1, keepdims=True) + epsilon)
    normed = lax.optimization_barrier((floats * inverse * norm_gain).astype(jnp.bfloat16))

    def activated(weight, scale):
        pre = jnp.dot(normed, weight, preferred_element_type=jnp.float32) * scale
        return lax.optimization_barrier(jnp.square(jax.nn.relu(pre)).astype(jnp.bfloat16))

    early_hidden = activated(early, up_scale[:early_width])
    late_up = gathered[:, rows:].reshape(-1, late_rows, parts, LATE)
    late_up = late_up.transpose(0, 2, 1, 3).reshape(-1, LATE)
    late_hidden = activated(late_up, up_scale[early_width:])
    hidden = jnp.concatenate([early_hidden, late_hidden], axis=1)

    core = lax.axis_index("c")
    cores, chips = lax.axis_size("c"), lax.axis_size("x")
    columns = down_scale.shape[0] * lax.axis_size("z") * lax.axis_size("y") // (cores * chips)
    theirs = down_blocks(1 - core, hidden, gathered, rows, columns, chips, jnp.bfloat16)
    arrived = lax.ppermute(theirs, "c", [(0, 1), (1, 0)])
    mine = down_blocks(core, hidden, gathered, rows, columns, chips, jnp.float32)
    chip_sum = (mine + arrived.astype(jnp.float32)).astype(jnp.bfloat16)
    tiles = lax.all_to_all(chip_sum, "x", 0, 0, tiled=True).astype(jnp.float32)
    return ((tiles[0] + tiles[1]) + (tiles[2] + tiles[3])).astype(jnp.bfloat16)


def solution(mesh):
    split = Mesh(mesh.devices.reshape(16, 4, 4, 2), FS + TP)
    return jax.shard_map(
        local,
        mesh=split,
        in_specs=(P(FS, None), P(), P(FS, TP), P(TP), P(TP, FS), P(FS)),
        out_specs=P(FS, TP),
        check_vma=False,
    )
```

```python
import jax
import jax.numpy as jnp
from jax import lax
from jax.experimental import pallas as pl
from jax.experimental.pallas import tpu as pltpu
from jax.sharding import Mesh
from jax.sharding import PartitionSpec as P

FS = ("z", "y")
TP = ("x", "c")

epsilon = 1e-06

LATE = 256


def spread(array, axis):
    count = lax.axis_size(axis)
    copies = jnp.broadcast_to(array[None], (count,) + array.shape)
    return lax.all_to_all(copies, axis, 0, 0, tiled=True)


def prepare_kernel(up_ref, down_ref, scale_ref, copies_ref, early_ref):
    rows, width = down_ref.shape
    early_width = early_ref.shape[1]
    late_width = width - early_width
    late_rows = copies_ref.shape[1] - rows
    at = lax.broadcasted_iota(jnp.int32, (rows, rows), 0)
    to = lax.broadcasted_iota(jnp.int32, (rows, rows), 1)
    scale = jnp.sum(jnp.where(at == to, scale_ref[...], 0.0), axis=1, keepdims=True)
    down = (down_ref[...] * scale).astype(jnp.bfloat16)
    early_ref[...] = up_ref[:, :early_width].astype(jnp.bfloat16)
    for k in range(copies_ref.shape[0]):
        copies_ref[k, :rows, :] = down
        for i in range(rows // late_rows):
            copies_ref[k, rows:, i * late_width : (i + 1) * late_width] = up_ref[
                i * late_rows : (i + 1) * late_rows, early_width:
            ].astype(jnp.bfloat16)


def down_kernel(core_ref, early_ref, late_ref, gathered_ref, out_ref):
    blocks, _, columns = out_ref.shape
    early_width = early_ref.shape[1]
    depth = gathered_ref.shape[2]
    groups = gathered_ref.shape[0] // (2 * blocks)
    rows = columns // groups
    contract = (((1,), (1,)), ((), ()))
    for i in range(blocks):
        first = (2 * i + core_ref[0]) * groups
        weight = gathered_ref[pl.ds(first, groups), 0:rows, :].reshape(columns, depth)
        total = lax.dot_general(
            early_ref[...], weight[:, :early_width], contract, preferred_element_type=jnp.float32
        ) + lax.dot_general(
            late_ref[...], weight[:, early_width:], contract, preferred_element_type=jnp.float32
        )
        out_ref[i] = total.astype(out_ref.dtype)


def down_blocks(core, early, late, gathered, columns, blocks, dtype):
    tokens = early.shape[0]
    depth = early.shape[1] + late.shape[1]
    vmem = pl.BlockSpec(memory_space=pltpu.VMEM)
    return pl.pallas_call(
        down_kernel,
        in_specs=[pl.BlockSpec(memory_space=pltpu.SMEM), vmem, vmem, vmem],
        out_specs=vmem,
        out_shape=jax.ShapeDtypeStruct((blocks, tokens, columns), dtype),
        cost_estimate=pl.CostEstimate(
            flops=2 * tokens * depth * columns * blocks,
            bytes_accessed=2 * (tokens * depth + columns * depth * blocks + tokens * columns * blocks),
            transcendentals=0,
        ),
        compiler_params=pltpu.CompilerParams(vmem_limit_bytes=24 * 2**20),
    )(core.reshape(1), early, late, gathered)


def local(tokens, norm_gain, up_weight, up_scale, down_weight, down_scale):
    rows, hidden_width = up_weight.shape
    early_width = hidden_width - LATE
    parts = hidden_width // LATE
    late_rows = rows // parts
    vmem = pl.BlockSpec(memory_space=pltpu.VMEM)
    copies, early = pl.pallas_call(
        prepare_kernel,
        in_specs=[vmem, vmem, vmem],
        out_specs=[vmem, vmem],
        out_shape=[
            jax.ShapeDtypeStruct(
                (lax.axis_size("y"), rows + late_rows, hidden_width), jnp.bfloat16
            ),
            jax.ShapeDtypeStruct((rows, early_width), jnp.bfloat16),
        ],
    )(up_weight, down_weight.T, down_scale.reshape(1, rows))
    both = lax.all_to_all(copies, "y", 0, 0, tiled=True)
    early, both = lax.optimization_barrier((early, both))
    gathered = lax.all_gather(both, "z", axis=0, tiled=True)
    early = lax.all_gather(early, "z", axis=0, tiled=False)
    early = spread(early, "y")
    early = early.transpose(1, 0, 2, 3).reshape(-1, early_width)

    floats = tokens.astype(jnp.float32)
    inverse = lax.rsqrt(jnp.mean(floats * floats, axis=-1, keepdims=True) + epsilon)
    normed = lax.optimization_barrier((floats * inverse * norm_gain).astype(jnp.bfloat16))

    def activated(weight, scale):
        pre = jnp.dot(normed, weight, preferred_element_type=jnp.float32) * scale
        return lax.optimization_barrier(jnp.square(jax.nn.relu(pre)).astype(jnp.bfloat16))

    early_hidden = activated(early, up_scale[:early_width])
    late_up = gathered[:, rows:].reshape(-1, late_rows, parts, LATE)
    late_up = late_up.transpose(0, 2, 1, 3).reshape(-1, LATE)
    late_hidden = activated(late_up, up_scale[early_width:])
    core = lax.axis_index("c")
    cores, chips = lax.axis_size("c"), lax.axis_size("x")
    columns = down_scale.shape[0] * lax.axis_size("z") * lax.axis_size("y") // (cores * chips)
    theirs = down_blocks(1 - core, early_hidden, late_hidden, gathered, columns, chips, jnp.bfloat16)
    arrived = lax.ppermute(theirs, "c", [(0, 1), (1, 0)])
    mine = down_blocks(core, early_hidden, late_hidden, gathered, columns, chips, jnp.float32)
    chip_sum = (mine + arrived.astype(jnp.float32)).astype(jnp.bfloat16)
    tiles = lax.all_to_all(chip_sum, "x", 0, 0, tiled=True).astype(jnp.float32)
    return ((tiles[0] + tiles[1]) + (tiles[2] + tiles[3])).astype(jnp.bfloat16)


def solution(mesh):
    split = Mesh(mesh.devices.reshape(16, 4, 4, 2), FS + TP)
    return jax.shard_map(
        local,
        mesh=split,
        in_specs=(P(FS, None), P(), P(FS, TP), P(TP), P(TP, FS), P(FS)),
        out_specs=P(FS, TP),
        check_vma=False,
    )
```

```python
import jax
import jax.numpy as jnp
from jax import lax
from jax.experimental import pallas as pl
from jax.experimental.pallas import tpu as pltpu
from jax.sharding import Mesh
from jax.sharding import PartitionSpec as P

FS = ("z", "y")
TP = ("x", "c")

epsilon = 1e-06

LATE = 256


def early_kernel(place_ref, normed_ref, own_ref, one_ref, two_ref, three_ref, scale_ref, out_ref, weight_ref):
    groups, members, rows, width = weight_ref.shape
    for d, block in enumerate((own_ref, one_ref, two_ref, three_ref)):
        member = lax.rem(place_ref[0] + members - d, members)
        weight_ref[:, pl.ds(member, 1)] = block[...].reshape(groups, 1, rows, width)
    pre = jnp.dot(
        normed_ref[...],
        weight_ref[...].reshape(groups * members * rows, width),
        preferred_element_type=jnp.float32,
    )
    kept = jnp.maximum(pre * scale_ref[...], 0.0)
    out_ref[...] = (kept * kept).astype(out_ref.dtype)


def early_block(place, normed, blocks, scale):
    groups, rows, width = blocks[0].shape
    vmem = pl.BlockSpec(memory_space=pltpu.VMEM)
    tokens, features = normed.shape
    return pl.pallas_call(
        early_kernel,
        in_specs=[pl.BlockSpec(memory_space=pltpu.SMEM)] + [vmem] * (2 + len(blocks)),
        out_specs=vmem,
        out_shape=jax.ShapeDtypeStruct((tokens, width), jnp.bfloat16),
        scratch_shapes=[pltpu.VMEM((groups, len(blocks), rows, width), jnp.bfloat16)],
        cost_estimate=pl.CostEstimate(
            flops=2 * tokens * features * width,
            bytes_accessed=2 * (tokens * features + features * width + tokens * width),
            transcendentals=0,
        ),
        compiler_params=pltpu.CompilerParams(vmem_limit_bytes=20 * 2**20),
    )(place.reshape(1), normed, *blocks, scale.reshape(1, width))


def prepare_kernel(up_ref, down_ref, scale_ref, copies_ref, early_ref):
    rows, width = down_ref.shape
    early_width = early_ref.shape[1]
    late_width = width - early_width
    late_rows = copies_ref.shape[1] - rows
    at = lax.broadcasted_iota(jnp.int32, (rows, rows), 0)
    to = lax.broadcasted_iota(jnp.int32, (rows, rows), 1)
    scale = jnp.sum(jnp.where(at == to, scale_ref[...], 0.0), axis=1, keepdims=True)
    down = (down_ref[...] * scale).astype(jnp.bfloat16)
    early_ref[...] = up_ref[:, :early_width].astype(jnp.bfloat16)
    for k in range(copies_ref.shape[0]):
        copies_ref[k, :rows, :] = down
        for i in range(rows // late_rows):
            copies_ref[k, rows:, i * late_width : (i + 1) * late_width] = up_ref[
                i * late_rows : (i + 1) * late_rows, early_width:
            ].astype(jnp.bfloat16)


def down_kernel(core_ref, early_ref, late_ref, gathered_ref, out_ref):
    blocks, _, columns = out_ref.shape
    early_width = early_ref.shape[1]
    depth = gathered_ref.shape[2]
    groups = gathered_ref.shape[0] // (2 * blocks)
    rows = columns // groups
    contract = (((1,), (1,)), ((), ()))
    for i in range(blocks):
        first = (2 * i + core_ref[0]) * groups
        weight = gathered_ref[pl.ds(first, groups), 0:rows, :].reshape(columns, depth)
        total = lax.dot_general(
            early_ref[...], weight[:, :early_width], contract, preferred_element_type=jnp.float32
        ) + lax.dot_general(
            late_ref[...], weight[:, early_width:], contract, preferred_element_type=jnp.float32
        )
        out_ref[i] = total.astype(out_ref.dtype)


def down_blocks(core, early, late, gathered, columns, blocks, dtype):
    tokens = early.shape[0]
    depth = early.shape[1] + late.shape[1]
    vmem = pl.BlockSpec(memory_space=pltpu.VMEM)
    return pl.pallas_call(
        down_kernel,
        in_specs=[pl.BlockSpec(memory_space=pltpu.SMEM), vmem, vmem, vmem],
        out_specs=vmem,
        out_shape=jax.ShapeDtypeStruct((blocks, tokens, columns), dtype),
        cost_estimate=pl.CostEstimate(
            flops=2 * tokens * depth * columns * blocks,
            bytes_accessed=2 * (tokens * depth + columns * depth * blocks + tokens * columns * blocks),
            transcendentals=0,
        ),
        compiler_params=pltpu.CompilerParams(vmem_limit_bytes=20 * 2**20),
    )(core.reshape(1), early, late, gathered)


def local(tokens, norm_gain, up_weight, up_scale, down_weight, down_scale):
    rows, hidden_width = up_weight.shape
    early_width = hidden_width - LATE
    parts = hidden_width // LATE
    late_rows = rows // parts
    vmem = pl.BlockSpec(memory_space=pltpu.VMEM)
    copies, early = pl.pallas_call(
        prepare_kernel,
        in_specs=[vmem, vmem, vmem],
        out_specs=[vmem, vmem],
        out_shape=[
            jax.ShapeDtypeStruct(
                (lax.axis_size("y"), rows + late_rows, hidden_width), jnp.bfloat16
            ),
            jax.ShapeDtypeStruct((rows, early_width), jnp.bfloat16),
        ],
    )(up_weight, down_weight.T, down_scale.reshape(1, rows))
    both = lax.all_to_all(copies, "y", 0, 0, tiled=True)
    early, both = lax.optimization_barrier((early, both))
    gathered = lax.all_gather(both, "z", axis=0, tiled=True)
    early = lax.all_gather(early, "z", axis=0, tiled=False)
    early, tokens = lax.optimization_barrier((early, tokens))
    members = lax.axis_size("y")

    def sent(d):
        return lax.ppermute(early, "y", [(i, (i + d) % members) for i in range(members)])

    two, one, three = sent(2), sent(1), sent(3)

    floats = tokens.astype(jnp.float32)
    inverse = lax.rsqrt(jnp.mean(floats * floats, axis=-1, keepdims=True) + epsilon)
    normed = lax.optimization_barrier((floats * inverse * norm_gain).astype(jnp.bfloat16))

    def activated(weight, scale):
        pre = jnp.dot(normed, weight, preferred_element_type=jnp.float32) * scale
        return lax.optimization_barrier(jnp.square(jax.nn.relu(pre)).astype(jnp.bfloat16))

    early_hidden = early_block(
        lax.axis_index("y"), normed, (early, one, two, three), up_scale[:early_width]
    )
    late_up = gathered[:, rows:].reshape(-1, late_rows, parts, LATE)
    late_up = late_up.transpose(0, 2, 1, 3).reshape(-1, LATE)
    late_hidden = activated(late_up, up_scale[early_width:])
    core = lax.axis_index("c")
    cores, chips = lax.axis_size("c"), lax.axis_size("x")
    columns = down_scale.shape[0] * lax.axis_size("z") * lax.axis_size("y") // (cores * chips)
    theirs = down_blocks(1 - core, early_hidden, late_hidden, gathered, columns, chips, jnp.bfloat16)
    arrived = lax.ppermute(theirs, "c", [(0, 1), (1, 0)])
    mine = down_blocks(core, early_hidden, late_hidden, gathered, columns, chips, jnp.float32)
    chip_sum = (mine + arrived.astype(jnp.float32)).astype(jnp.bfloat16)
    tiles = lax.all_to_all(chip_sum, "x", 0, 0, tiled=True).astype(jnp.float32)
    return ((tiles[0] + tiles[1]) + (tiles[2] + tiles[3])).astype(jnp.bfloat16)


def solution(mesh):
    split = Mesh(mesh.devices.reshape(16, 4, 4, 2), FS + TP)
    return jax.shard_map(
        local,
        mesh=split,
        in_specs=(P(FS, None), P(), P(FS, TP), P(TP), P(TP, FS), P(FS)),
        out_specs=P(FS, TP),
        check_vma=False,
    )
```

```python
import jax
import jax.numpy as jnp
from jax import lax
from jax.experimental import pallas as pl
from jax.experimental.pallas import tpu as pltpu
from jax.sharding import Mesh
from jax.sharding import PartitionSpec as P

FS = ("z", "y")
TP = ("x", "c")

epsilon = 1e-06

LATE = 256
THEIRS_VMEM = 44 * 2**20


def early_kernel(place_ref, normed_ref, own_ref, one_ref, two_ref, three_ref, scale_ref, out_ref, weight_ref):
    groups, members, rows, width = weight_ref.shape
    for d, block in enumerate((own_ref, one_ref, two_ref, three_ref)):
        member = lax.rem(place_ref[0] + members - d, members)
        weight_ref[:, pl.ds(member, 1)] = block[...].reshape(groups, 1, rows, width)
    pre = jnp.dot(
        normed_ref[...],
        weight_ref[...].reshape(groups * members * rows, width),
        preferred_element_type=jnp.float32,
    )
    kept = jnp.maximum(pre * scale_ref[...], 0.0)
    out_ref[...] = (kept * kept).astype(out_ref.dtype)


def early_block(place, normed, blocks, scale):
    groups, rows, width = blocks[0].shape
    vmem = pl.BlockSpec(memory_space=pltpu.VMEM)
    tokens, features = normed.shape
    return pl.pallas_call(
        early_kernel,
        in_specs=[pl.BlockSpec(memory_space=pltpu.SMEM)] + [vmem] * (2 + len(blocks)),
        out_specs=vmem,
        out_shape=jax.ShapeDtypeStruct((tokens, width), jnp.bfloat16),
        scratch_shapes=[pltpu.VMEM((groups, len(blocks), rows, width), jnp.bfloat16)],
        cost_estimate=pl.CostEstimate(
            flops=2 * tokens * features * width,
            bytes_accessed=2 * (tokens * features + features * width + tokens * width),
            transcendentals=0,
        ),
        compiler_params=pltpu.CompilerParams(vmem_limit_bytes=20 * 2**20),
    )(place.reshape(1), normed, *blocks, scale.reshape(1, width))


def prepare_kernel(up_ref, down_ref, scale_ref, copies_ref, early_ref):
    rows, width = down_ref.shape
    early_width = early_ref.shape[1]
    late_width = width - early_width
    late_rows = copies_ref.shape[1] - rows
    at = lax.broadcasted_iota(jnp.int32, (rows, rows), 0)
    to = lax.broadcasted_iota(jnp.int32, (rows, rows), 1)
    scale = jnp.sum(jnp.where(at == to, scale_ref[...], 0.0), axis=1, keepdims=True)
    down = (down_ref[...] * scale).astype(jnp.bfloat16)
    early_ref[...] = up_ref[:, :early_width].astype(jnp.bfloat16)
    for k in range(copies_ref.shape[0]):
        copies_ref[k, :rows, :] = down
        for i in range(rows // late_rows):
            copies_ref[k, rows:, i * late_width : (i + 1) * late_width] = up_ref[
                i * late_rows : (i + 1) * late_rows, early_width:
            ].astype(jnp.bfloat16)


def products(early, late, weight):
    early_width = early.shape[1]
    contract = (((1,), (1,)), ((), ()))
    return lax.dot_general(
        early, weight[:, :early_width], contract, preferred_element_type=jnp.float32
    ) + lax.dot_general(
        late, weight[:, early_width:], contract, preferred_element_type=jnp.float32
    )


def theirs_kernel(
    core_ref, early_ref, normed_ref, scale_ref, gathered_ref,
    theirs_ref, late_ref, kept_ref,
    rows_ref, late_weight_ref, weight_ref, sems,
):
    blocks, groups, rows, depth = kept_ref.shape
    places, late_rows, _ = rows_ref.shape
    late_width = late_ref.shape[1]
    core = core_ref[0]

    def block(i, side):
        first = (2 * i + side) * groups
        return gathered_ref.at[pl.ds(first, groups), pl.ds(0, rows)]

    late_copy = pltpu.make_async_copy(
        gathered_ref.at[:, pl.ds(rows, late_rows)], rows_ref, sems.at[2 * blocks]
    )
    late_copy.start()
    sending = [
        pltpu.make_async_copy(block(i, 1 - core), weight_ref.at[i], sems.at[i])
        for i in range(blocks)
    ]
    keeping = [
        pltpu.make_async_copy(block(i, core), kept_ref.at[i], sems.at[blocks + i])
        for i in range(blocks)
    ]
    for copy in sending + keeping:
        copy.start()
    late_copy.wait()
    for i in range(rows // late_rows):
        late_weight_ref[:, i * late_rows : (i + 1) * late_rows, :] = rows_ref[
            :, :, i * late_width : (i + 1) * late_width
        ]
    pre = jnp.dot(
        normed_ref[...],
        late_weight_ref[...].reshape(places * rows, late_width),
        preferred_element_type=jnp.float32,
    )
    kept = jnp.maximum(pre * scale_ref[...], 0.0)
    late_ref[...] = (kept * kept).astype(late_ref.dtype)
    for i in range(blocks):
        sending[i].wait()
        weight = weight_ref[i].reshape(groups * rows, depth)
        theirs_ref[i] = products(early_ref[...], late_ref[...], weight).astype(theirs_ref.dtype)
    for copy in keeping:
        copy.wait()


def theirs_blocks(core, early, normed, scale, gathered, rows, columns, blocks):
    tokens, features = normed.shape
    places, _, depth = gathered.shape
    groups = columns // rows
    late_rows = gathered.shape[1] - rows
    width = scale.shape[0]
    vmem = pl.BlockSpec(memory_space=pltpu.VMEM)
    weights = (blocks, groups, rows, depth)
    return pl.pallas_call(
        theirs_kernel,
        in_specs=[
            pl.BlockSpec(memory_space=pltpu.SMEM), vmem, vmem, vmem,
            pl.BlockSpec(memory_space=pltpu.HBM),
        ],
        out_specs=[vmem] * 3,
        out_shape=[
            jax.ShapeDtypeStruct((blocks, tokens, columns), jnp.bfloat16),
            jax.ShapeDtypeStruct((tokens, width), jnp.bfloat16),
            jax.ShapeDtypeStruct(weights, jnp.bfloat16),
        ],
        scratch_shapes=[
            pltpu.VMEM((places, late_rows, depth), jnp.bfloat16),
            pltpu.VMEM((places, rows, width), jnp.bfloat16),
            pltpu.VMEM(weights, jnp.bfloat16),
            pltpu.SemaphoreType.DMA((2 * blocks + 1,)),
        ],
        cost_estimate=pl.CostEstimate(
            flops=2 * tokens * (depth * columns * blocks + features * width),
            bytes_accessed=2 * (tokens * features + 2 * columns * depth * blocks),
            transcendentals=0,
        ),
        compiler_params=pltpu.CompilerParams(vmem_limit_bytes=THEIRS_VMEM),
    )(core.reshape(1), early, normed, scale.reshape(1, width), gathered)


def mine_kernel(early_ref, late_ref, weight_ref, out_ref):
    blocks, groups, rows, depth = weight_ref.shape
    for i in range(blocks):
        weight = weight_ref[i].reshape(groups * rows, depth)
        out_ref[i] = products(early_ref[...], late_ref[...], weight)


def mine_blocks(early, late, weights):
    blocks, groups, rows, depth = weights.shape
    tokens = early.shape[0]
    vmem = pl.BlockSpec(memory_space=pltpu.VMEM)
    return pl.pallas_call(
        mine_kernel,
        in_specs=[vmem] * 3,
        out_specs=vmem,
        out_shape=jax.ShapeDtypeStruct((blocks, tokens, groups * rows), jnp.float32),
        cost_estimate=pl.CostEstimate(
            flops=2 * tokens * depth * groups * rows * blocks,
            bytes_accessed=2 * (tokens * depth + groups * rows * depth * blocks),
            transcendentals=0,
        ),
        compiler_params=pltpu.CompilerParams(vmem_limit_bytes=16 * 2**20),
    )(early, late, weights)


def local(tokens, norm_gain, up_weight, up_scale, down_weight, down_scale):
    rows, hidden_width = up_weight.shape
    early_width = hidden_width - LATE
    parts = hidden_width // LATE
    late_rows = rows // parts
    vmem = pl.BlockSpec(memory_space=pltpu.VMEM)
    copies, early = pl.pallas_call(
        prepare_kernel,
        in_specs=[vmem, vmem, vmem],
        out_specs=[vmem, vmem],
        out_shape=[
            jax.ShapeDtypeStruct(
                (lax.axis_size("y"), rows + late_rows, hidden_width), jnp.bfloat16
            ),
            jax.ShapeDtypeStruct((rows, early_width), jnp.bfloat16),
        ],
    )(up_weight, down_weight.T, down_scale.reshape(1, rows))
    both = lax.all_to_all(copies, "y", 0, 0, tiled=True)
    early, both = lax.optimization_barrier((early, both))
    gathered = lax.all_gather(both, "z", axis=0, tiled=True)
    early = lax.all_gather(early, "z", axis=0, tiled=False)
    early, tokens, up_scale = lax.optimization_barrier((early, tokens, up_scale))
    members = lax.axis_size("y")

    def sent(d):
        return lax.ppermute(early, "y", [(i, (i + d) % members) for i in range(members)])

    two, one, three = sent(2), sent(1), sent(3)

    floats = tokens.astype(jnp.float32)
    inverse = lax.rsqrt(jnp.mean(floats * floats, axis=-1, keepdims=True) + epsilon)
    normed = lax.optimization_barrier((floats * inverse * norm_gain).astype(jnp.bfloat16))

    early_hidden = early_block(
        lax.axis_index("y"), normed, (early, one, two, three), up_scale[:early_width]
    )
    core = lax.axis_index("c")
    cores, chips = lax.axis_size("c"), lax.axis_size("x")
    columns = rows * lax.axis_size("z") * lax.axis_size("y") // (cores * chips)
    theirs, late_hidden, kept = theirs_blocks(
        core, early_hidden, normed, up_scale[early_width:], gathered, rows, columns, chips
    )
    arrived = lax.ppermute(theirs, "c", [(0, 1), (1, 0)])
    mine = mine_blocks(early_hidden, late_hidden, kept)
    chip_sum = (mine + arrived.astype(jnp.float32)).astype(jnp.bfloat16)
    tiles = lax.all_to_all(chip_sum, "x", 0, 0, tiled=True).astype(jnp.float32)
    return ((tiles[0] + tiles[1]) + (tiles[2] + tiles[3])).astype(jnp.bfloat16)


def solution(mesh):
    split = Mesh(mesh.devices.reshape(16, 4, 4, 2), FS + TP)
    return jax.shard_map(
        local,
        mesh=split,
        in_specs=(P(FS, None), P(), P(FS, TP), P(TP), P(TP, FS), P(FS)),
        out_specs=P(FS, TP),
        check_vma=False,
    )
```

```python
import jax
import jax.numpy as jnp
from jax import lax
from jax.experimental import pallas as pl
from jax.experimental.pallas import tpu as pltpu
from jax.sharding import Mesh
from jax.sharding import PartitionSpec as P

FS = ("z", "y")
TP = ("x", "c")

epsilon = 1e-06

LATE = 256
TAIL_VMEM = 20 * 2**20
FETCH_VMEM = 48 * 2**20


def early_kernel(place_ref, normed_ref, own_ref, one_ref, two_ref, three_ref, scale_ref, out_ref, weight_ref):
    groups, members, rows, width = weight_ref.shape
    for d, block in enumerate((own_ref, one_ref, two_ref, three_ref)):
        member = lax.rem(place_ref[0] + members - d, members)
        weight_ref[:, pl.ds(member, 1)] = block[...].reshape(groups, 1, rows, width)
    pre = jnp.dot(
        normed_ref[...],
        weight_ref[...].reshape(groups * members * rows, width),
        preferred_element_type=jnp.float32,
    )
    kept = jnp.maximum(pre * scale_ref[...], 0.0)
    out_ref[...] = (kept * kept).astype(out_ref.dtype)


def early_block(place, normed, blocks, scale):
    groups, rows, width = blocks[0].shape
    vmem = pl.BlockSpec(memory_space=pltpu.VMEM)
    tokens, features = normed.shape
    return pl.pallas_call(
        early_kernel,
        in_specs=[pl.BlockSpec(memory_space=pltpu.SMEM)] + [vmem] * (2 + len(blocks)),
        out_specs=vmem,
        out_shape=jax.ShapeDtypeStruct((tokens, width), jnp.bfloat16),
        scratch_shapes=[pltpu.VMEM((groups, len(blocks), rows, width), jnp.bfloat16)],
        cost_estimate=pl.CostEstimate(
            flops=2 * tokens * features * width,
            bytes_accessed=2 * (tokens * features + features * width + tokens * width),
            transcendentals=0,
        ),
        compiler_params=pltpu.CompilerParams(vmem_limit_bytes=20 * 2**20),
    )(place.reshape(1), normed, *blocks, scale.reshape(1, width))


def prepare_kernel(up_ref, down_ref, scale_ref, copies_ref, early_ref):
    rows, width = down_ref.shape
    early_width = early_ref.shape[1]
    late_width = width - early_width
    late_rows = copies_ref.shape[1] - rows
    at = lax.broadcasted_iota(jnp.int32, (rows, rows), 0)
    to = lax.broadcasted_iota(jnp.int32, (rows, rows), 1)
    scale = jnp.sum(jnp.where(at == to, scale_ref[...], 0.0), axis=1, keepdims=True)
    down = (down_ref[...] * scale).astype(jnp.bfloat16)
    early_ref[...] = up_ref[:, :early_width].astype(jnp.bfloat16)
    for k in range(copies_ref.shape[0]):
        copies_ref[k, :rows, :] = down
        for i in range(rows // late_rows):
            copies_ref[k, rows:, i * late_width : (i + 1) * late_width] = up_ref[
                i * late_rows : (i + 1) * late_rows, early_width:
            ].astype(jnp.bfloat16)


def products(early, late, weight):
    early_width = early.shape[1]
    contract = (((1,), (1,)), ((), ()))
    return lax.dot_general(
        early, weight[:, :early_width], contract, preferred_element_type=jnp.float32
    ) + lax.dot_general(
        late, weight[:, early_width:], contract, preferred_element_type=jnp.float32
    )


def side_weight(down_ref, side, i, blocks, columns):
    groups = down_ref.shape[0] // (2 * blocks)
    first = (2 * i + side) * groups
    weight = down_ref[pl.ds(first, groups)]
    return weight.reshape(columns, down_ref.shape[2])


def fetch_kernel(gathered_ref, late_view_ref, down_ref, late_ref, sems):
    rows = down_ref.shape[1]
    late = pltpu.make_async_copy(
        late_view_ref.at[:, late_view_ref.shape[1] - 1], late_ref, sems.at[0]
    )
    down = pltpu.make_async_copy(gathered_ref.at[:, pl.ds(0, rows)], down_ref, sems.at[1])
    late.start()
    down.start()
    late.wait()
    down.wait()


def fetched(gathered, rows, width):
    places, all_rows, depth = gathered.shape
    late_rows = all_rows - rows
    parts = depth // width
    view = gathered.reshape(places, all_rows // late_rows, late_rows, parts, width)
    view = view.transpose(0, 1, 3, 2, 4)
    vmem = pl.BlockSpec(memory_space=pltpu.VMEM)
    hbm = pl.BlockSpec(memory_space=pltpu.HBM)
    down, late = pl.pallas_call(
        fetch_kernel,
        in_specs=[hbm, hbm],
        out_specs=[vmem, vmem],
        out_shape=[
            jax.ShapeDtypeStruct((places, rows, depth), gathered.dtype),
            jax.ShapeDtypeStruct((places, parts, late_rows, width), gathered.dtype),
        ],
        scratch_shapes=[pltpu.SemaphoreType.DMA((2,))],
        cost_estimate=pl.CostEstimate(
            flops=1000, bytes_accessed=4 * places * all_rows * depth, transcendentals=0
        ),
        compiler_params=pltpu.CompilerParams(vmem_limit_bytes=FETCH_VMEM),
    )(gathered, view)
    return down, late.reshape(-1, width)


def theirs_kernel(
    core_ref, early_ref, normed_ref, weight_ref, scale_ref, down_ref, theirs_ref, late_ref
):
    blocks, _, columns = theirs_ref.shape
    pre = jnp.dot(normed_ref[...], weight_ref[...], preferred_element_type=jnp.float32)
    kept = jnp.maximum(pre * scale_ref[...], 0.0)
    late_ref[...] = (kept * kept).astype(late_ref.dtype)
    for i in range(blocks):
        weight = side_weight(down_ref, 1 - core_ref[0], i, blocks, columns)
        theirs_ref[i] = products(early_ref[...], late_ref[...], weight).astype(theirs_ref.dtype)


def theirs_blocks(core, early, normed, late_weight, scale, down, columns, blocks):
    tokens, features = normed.shape
    depth = down.shape[2]
    width = scale.shape[0]
    vmem = pl.BlockSpec(memory_space=pltpu.VMEM)
    return pl.pallas_call(
        theirs_kernel,
        in_specs=[pl.BlockSpec(memory_space=pltpu.SMEM)] + [vmem] * 5,
        out_specs=[vmem] * 2,
        out_shape=[
            jax.ShapeDtypeStruct((blocks, tokens, columns), jnp.bfloat16),
            jax.ShapeDtypeStruct((tokens, width), jnp.bfloat16),
        ],
        cost_estimate=pl.CostEstimate(
            flops=2 * tokens * (depth * columns * blocks + features * width),
            bytes_accessed=2 * (tokens * features + columns * depth * blocks),
            transcendentals=0,
        ),
        compiler_params=pltpu.CompilerParams(vmem_limit_bytes=TAIL_VMEM),
    )(core.reshape(1), early, normed, late_weight, scale.reshape(1, width), down)


def mine_kernel(core_ref, early_ref, late_ref, down_ref, out_ref):
    blocks, _, columns = out_ref.shape
    for i in range(blocks):
        weight = side_weight(down_ref, core_ref[0], i, blocks, columns)
        out_ref[i] = products(early_ref[...], late_ref[...], weight)


def mine_blocks(core, early, late, down, columns, blocks):
    tokens = early.shape[0]
    depth = down.shape[2]
    vmem = pl.BlockSpec(memory_space=pltpu.VMEM)
    return pl.pallas_call(
        mine_kernel,
        in_specs=[pl.BlockSpec(memory_space=pltpu.SMEM)] + [vmem] * 3,
        out_specs=vmem,
        out_shape=jax.ShapeDtypeStruct((blocks, tokens, columns), jnp.float32),
        cost_estimate=pl.CostEstimate(
            flops=2 * tokens * depth * columns * blocks,
            bytes_accessed=2 * (tokens * depth + columns * depth * blocks),
            transcendentals=0,
        ),
        compiler_params=pltpu.CompilerParams(vmem_limit_bytes=TAIL_VMEM),
    )(core.reshape(1), early, late, down)


def local(tokens, norm_gain, up_weight, up_scale, down_weight, down_scale):
    rows, hidden_width = up_weight.shape
    early_width = hidden_width - LATE
    parts = hidden_width // LATE
    late_rows = rows // parts
    vmem = pl.BlockSpec(memory_space=pltpu.VMEM)
    copies, early = pl.pallas_call(
        prepare_kernel,
        in_specs=[vmem, vmem, vmem],
        out_specs=[vmem, vmem],
        out_shape=[
            jax.ShapeDtypeStruct(
                (lax.axis_size("y"), rows + late_rows, hidden_width), jnp.bfloat16
            ),
            jax.ShapeDtypeStruct((rows, early_width), jnp.bfloat16),
        ],
    )(up_weight, down_weight.T, down_scale.reshape(1, rows))
    both = lax.all_to_all(copies, "y", 0, 0, tiled=True)
    early, both = lax.optimization_barrier((early, both))
    gathered = lax.all_gather(both, "z", axis=0, tiled=True)
    early = lax.all_gather(early, "z", axis=0, tiled=False)
    early, tokens, up_scale = lax.optimization_barrier((early, tokens, up_scale))
    members = lax.axis_size("y")

    def sent(d):
        return lax.ppermute(early, "y", [(i, (i + d) % members) for i in range(members)])

    two, one, three = sent(2), sent(1), sent(3)

    floats = tokens.astype(jnp.float32)
    inverse = lax.rsqrt(jnp.mean(floats * floats, axis=-1, keepdims=True) + epsilon)
    normed = lax.optimization_barrier((floats * inverse * norm_gain).astype(jnp.bfloat16))

    early_hidden = early_block(
        lax.axis_index("y"), normed, (early, one, two, three), up_scale[:early_width]
    )
    core = lax.axis_index("c")
    cores, chips = lax.axis_size("c"), lax.axis_size("x")
    columns = rows * lax.axis_size("z") * lax.axis_size("y") // (cores * chips)
    down, late_weight = fetched(gathered, rows, LATE)
    theirs, late_hidden = theirs_blocks(
        core, early_hidden, normed, late_weight, up_scale[early_width:], down, columns, chips
    )
    arrived = lax.ppermute(theirs, "c", [(0, 1), (1, 0)])
    mine = mine_blocks(core, early_hidden, late_hidden, down, columns, chips)
    chip_sum = (mine + arrived.astype(jnp.float32)).astype(jnp.bfloat16)
    tiles = lax.all_to_all(chip_sum, "x", 0, 0, tiled=True).astype(jnp.float32)
    return ((tiles[0] + tiles[1]) + (tiles[2] + tiles[3])).astype(jnp.bfloat16)


def solution(mesh):
    split = Mesh(mesh.devices.reshape(16, 4, 4, 2), FS + TP)
    return jax.shard_map(
        local,
        mesh=split,
        in_specs=(P(FS, None), P(), P(FS, TP), P(TP), P(TP, FS), P(FS)),
        out_specs=P(FS, TP),
        check_vma=False,
    )
```

```python
import jax
import jax.numpy as jnp
from jax import lax
from jax.experimental import pallas as pl
from jax.experimental.pallas import tpu as pltpu
from jax.sharding import Mesh
from jax.sharding import PartitionSpec as P

FS = ("z", "y")
TP = ("x", "c")

epsilon = 1e-06

LATE = 256
TAIL_VMEM = 20 * 2**20
FETCH_VMEM = 48 * 2**20


def early_kernel(place_ref, normed_ref, own_ref, one_ref, two_ref, three_ref, scale_ref, out_ref, weight_ref):
    groups, members, rows, width = weight_ref.shape
    for d, block in enumerate((own_ref, one_ref, two_ref, three_ref)):
        member = lax.rem(place_ref[0] + members - d, members)
        weight_ref[:, pl.ds(member, 1)] = block[...].reshape(groups, 1, rows, width)
    pre = jnp.dot(
        normed_ref[...],
        weight_ref[...].reshape(groups * members * rows, width),
        preferred_element_type=jnp.float32,
    )
    kept = jnp.maximum(pre * scale_ref[...], 0.0)
    out_ref[...] = (kept * kept).astype(out_ref.dtype)


def early_block(place, normed, blocks, scale):
    groups, rows, width = blocks[0].shape
    vmem = pl.BlockSpec(memory_space=pltpu.VMEM)
    tokens, features = normed.shape
    return pl.pallas_call(
        early_kernel,
        in_specs=[pl.BlockSpec(memory_space=pltpu.SMEM)] + [vmem] * (2 + len(blocks)),
        out_specs=vmem,
        out_shape=jax.ShapeDtypeStruct((tokens, width), jnp.bfloat16),
        scratch_shapes=[pltpu.VMEM((groups, len(blocks), rows, width), jnp.bfloat16)],
        cost_estimate=pl.CostEstimate(
            flops=2 * tokens * features * width,
            bytes_accessed=2 * (tokens * features + features * width + tokens * width),
            transcendentals=0,
        ),
        compiler_params=pltpu.CompilerParams(vmem_limit_bytes=20 * 2**20),
    )(place, normed, *blocks, scale.reshape(1, width))


def prepare_kernel(up_ref, down_ref, scale_ref, copies_ref, early_ref):
    rows, width = down_ref.shape
    early_width = early_ref.shape[1]
    late_width = width - early_width
    late_rows = copies_ref.shape[1] - rows
    at = lax.broadcasted_iota(jnp.int32, (rows, rows), 0)
    to = lax.broadcasted_iota(jnp.int32, (rows, rows), 1)
    scale = jnp.sum(jnp.where(at == to, scale_ref[...], 0.0), axis=1, keepdims=True)
    down = (down_ref[...] * scale).astype(jnp.bfloat16)
    early_ref[...] = up_ref[:, :early_width].astype(jnp.bfloat16)
    for k in range(copies_ref.shape[0]):
        copies_ref[k, :rows, :] = down
        for i in range(rows // late_rows):
            copies_ref[k, rows:, i * late_width : (i + 1) * late_width] = up_ref[
                i * late_rows : (i + 1) * late_rows, early_width:
            ].astype(jnp.bfloat16)


def products(early, late, weight):
    early_width = early.shape[1]
    contract = (((1,), (1,)), ((), ()))
    return lax.dot_general(
        early, weight[:, :early_width], contract, preferred_element_type=jnp.float32
    ) + lax.dot_general(
        late, weight[:, early_width:], contract, preferred_element_type=jnp.float32
    )


def side_weight(down_ref, side, i, blocks, columns):
    groups = down_ref.shape[0] // (2 * blocks)
    first = (2 * i + side) * groups
    weight = down_ref[pl.ds(first, groups)]
    return weight.reshape(columns, down_ref.shape[2])


def fetch_kernel(gathered_ref, late_view_ref, down_ref, late_ref, sems):
    rows = down_ref.shape[1]
    late = pltpu.make_async_copy(
        late_view_ref.at[:, late_view_ref.shape[1] - 1], late_ref, sems.at[0]
    )
    down = pltpu.make_async_copy(gathered_ref.at[:, pl.ds(0, rows)], down_ref, sems.at[1])
    late.start()
    down.start()
    late.wait()
    down.wait()


def fetched(gathered, rows, width):
    places, all_rows, depth = gathered.shape
    late_rows = all_rows - rows
    parts = depth // width
    view = gathered.reshape(places, all_rows // late_rows, late_rows, parts, width)
    view = view.transpose(0, 1, 3, 2, 4)
    vmem = pl.BlockSpec(memory_space=pltpu.VMEM)
    hbm = pl.BlockSpec(memory_space=pltpu.HBM)
    down, late = pl.pallas_call(
        fetch_kernel,
        in_specs=[hbm, hbm],
        out_specs=[vmem, vmem],
        out_shape=[
            jax.ShapeDtypeStruct((places, rows, depth), gathered.dtype),
            jax.ShapeDtypeStruct((places, parts, late_rows, width), gathered.dtype),
        ],
        scratch_shapes=[pltpu.SemaphoreType.DMA((2,))],
        cost_estimate=pl.CostEstimate(
            flops=1000, bytes_accessed=4 * places * all_rows * depth, transcendentals=0
        ),
        compiler_params=pltpu.CompilerParams(vmem_limit_bytes=FETCH_VMEM),
    )(gathered, view)
    return down, late.reshape(-1, width)


def theirs_kernel(
    core_ref, early_ref, normed_ref, weight_ref, scale_ref, down_ref, theirs_ref, late_ref
):
    blocks, _, columns = theirs_ref.shape
    pre = jnp.dot(normed_ref[...], weight_ref[...], preferred_element_type=jnp.float32)
    kept = jnp.maximum(pre * scale_ref[...], 0.0)
    late_ref[...] = (kept * kept).astype(late_ref.dtype)
    for i in range(blocks):
        weight = side_weight(down_ref, 1 - core_ref[1], i, blocks, columns)
        theirs_ref[i] = products(early_ref[...], late_ref[...], weight).astype(theirs_ref.dtype)


def theirs_blocks(core, early, normed, late_weight, scale, down, columns, blocks):
    tokens, features = normed.shape
    depth = down.shape[2]
    width = scale.shape[0]
    vmem = pl.BlockSpec(memory_space=pltpu.VMEM)
    return pl.pallas_call(
        theirs_kernel,
        in_specs=[pl.BlockSpec(memory_space=pltpu.SMEM)] + [vmem] * 5,
        out_specs=[vmem] * 2,
        out_shape=[
            jax.ShapeDtypeStruct((blocks, tokens, columns), jnp.bfloat16),
            jax.ShapeDtypeStruct((tokens, width), jnp.bfloat16),
        ],
        cost_estimate=pl.CostEstimate(
            flops=2 * tokens * (depth * columns * blocks + features * width),
            bytes_accessed=2 * (tokens * features + columns * depth * blocks),
            transcendentals=0,
        ),
        compiler_params=pltpu.CompilerParams(vmem_limit_bytes=TAIL_VMEM),
    )(core, early, normed, late_weight, scale.reshape(1, width), down)


def mine_kernel(core_ref, early_ref, late_ref, down_ref, out_ref):
    blocks, _, columns = out_ref.shape
    for i in range(blocks):
        weight = side_weight(down_ref, core_ref[1], i, blocks, columns)
        out_ref[i] = products(early_ref[...], late_ref[...], weight)


def mine_blocks(core, early, late, down, columns, blocks):
    tokens = early.shape[0]
    depth = down.shape[2]
    vmem = pl.BlockSpec(memory_space=pltpu.VMEM)
    return pl.pallas_call(
        mine_kernel,
        in_specs=[pl.BlockSpec(memory_space=pltpu.SMEM)] + [vmem] * 3,
        out_specs=vmem,
        out_shape=jax.ShapeDtypeStruct((blocks, tokens, columns), jnp.float32),
        cost_estimate=pl.CostEstimate(
            flops=2 * tokens * depth * columns * blocks,
            bytes_accessed=2 * (tokens * depth + columns * depth * blocks),
            transcendentals=0,
        ),
        compiler_params=pltpu.CompilerParams(vmem_limit_bytes=TAIL_VMEM),
    )(core, early, late, down)


def add_kernel(place_ref, mine_ref, arrived_ref, direct_ref, *turn_refs):
    blocks, early_tokens, _ = direct_ref.shape
    for i in range(blocks):
        total = mine_ref[i, :early_tokens] + arrived_ref[i, :early_tokens].astype(jnp.float32)
        direct_ref[i] = total.astype(direct_ref.dtype)
    for d, turn_ref in enumerate(turn_refs):
        i = lax.rem(place_ref[2] + d, blocks)
        total = mine_ref[i, early_tokens:] + arrived_ref[i, early_tokens:].astype(jnp.float32)
        turn_ref[...] = total.astype(turn_ref.dtype)


def added(place, mine, arrived):
    blocks, tokens, columns = mine.shape
    early_tokens = tokens // 2
    vmem = pl.BlockSpec(memory_space=pltpu.VMEM)
    turn = jax.ShapeDtypeStruct((tokens - early_tokens, columns), arrived.dtype)
    direct = jax.ShapeDtypeStruct((blocks, early_tokens, columns), arrived.dtype)
    return pl.pallas_call(
        add_kernel,
        in_specs=[pl.BlockSpec(memory_space=pltpu.SMEM), vmem, vmem],
        out_specs=[vmem] * (1 + blocks),
        out_shape=[direct] + [turn] * blocks,
        compiler_params=pltpu.CompilerParams(vmem_limit_bytes=TAIL_VMEM),
    )(place, mine, arrived)


def sum_kernel(tiles_ref, *refs):
    out_ref = refs[-1]
    blocks, early_tokens, _ = tiles_ref.shape
    total = tiles_ref[0].astype(jnp.float32)
    for i in range(1, blocks):
        total = total + tiles_ref[i].astype(jnp.float32)
    out_ref[:early_tokens, :] = total.astype(out_ref.dtype)
    total = refs[0][...].astype(jnp.float32)
    for turn_ref in refs[1:-1]:
        total = total + turn_ref[...].astype(jnp.float32)
    out_ref[early_tokens:, :] = total.astype(out_ref.dtype)


def local(tokens, norm_gain, up_weight, up_scale, down_weight, down_scale):
    rows, hidden_width = up_weight.shape
    early_width = hidden_width - LATE
    parts = hidden_width // LATE
    late_rows = rows // parts
    vmem = pl.BlockSpec(memory_space=pltpu.VMEM)
    copies, early = pl.pallas_call(
        prepare_kernel,
        in_specs=[vmem, vmem, vmem],
        out_specs=[vmem, vmem],
        out_shape=[
            jax.ShapeDtypeStruct(
                (lax.axis_size("y"), rows + late_rows, hidden_width), jnp.bfloat16
            ),
            jax.ShapeDtypeStruct((rows, early_width), jnp.bfloat16),
        ],
    )(up_weight, down_weight.T, down_scale.reshape(1, rows))
    both = lax.all_to_all(copies, "y", 0, 0, tiled=True)
    early, both = lax.optimization_barrier((early, both))
    gathered = lax.all_gather(both, "z", axis=0, tiled=True)
    early = lax.all_gather(early, "z", axis=0, tiled=False)
    early, tokens, up_scale = lax.optimization_barrier((early, tokens, up_scale))
    members = lax.axis_size("y")
    places = jnp.stack([lax.axis_index("y"), lax.axis_index("c"), lax.axis_index("x")])

    def sent(d):
        return lax.ppermute(early, "y", [(i, (i + d) % members) for i in range(members)])

    two, one, three = sent(2), sent(1), sent(3)

    floats = tokens.astype(jnp.float32)
    inverse = lax.rsqrt(jnp.mean(floats * floats, axis=-1, keepdims=True) + epsilon)
    normed = lax.optimization_barrier((floats * inverse * norm_gain).astype(jnp.bfloat16))

    early_hidden = early_block(
        places, normed, (early, one, two, three), up_scale[:early_width]
    )
    cores, chips = lax.axis_size("c"), lax.axis_size("x")
    columns = rows * lax.axis_size("z") * lax.axis_size("y") // (cores * chips)
    down, late_weight = fetched(gathered, rows, LATE)
    theirs, late_hidden = theirs_blocks(
        places, early_hidden, normed, late_weight, up_scale[early_width:], down, columns, chips
    )
    arrived = lax.ppermute(theirs, "c", [(0, 1), (1, 0)])
    mine = mine_blocks(places, early_hidden, late_hidden, down, columns, chips)
    direct, own, *turns = added(places, mine, arrived)
    tiles = lax.all_to_all(direct, "x", 0, 0, tiled=True)

    def turned(block, d):
        return lax.ppermute(block, "x", [(i, (i + d) % chips) for i in range(chips)])

    turns = [turned(block, d + 1) for d, block in enumerate(turns)]
    return pl.pallas_call(
        sum_kernel,
        in_specs=[vmem] * (1 + chips),
        out_specs=vmem,
        out_shape=jax.ShapeDtypeStruct((tokens.shape[0], columns), jnp.bfloat16),
        compiler_params=pltpu.CompilerParams(vmem_limit_bytes=TAIL_VMEM),
    )(tiles, own, *turns)


def solution(mesh):
    split = Mesh(mesh.devices.reshape(16, 4, 4, 2), FS + TP)
    return jax.shard_map(
        local,
        mesh=split,
        in_specs=(P(FS, None), P(), P(FS, TP), P(TP), P(TP, FS), P(FS)),
        out_specs=P(FS, TP),
        check_vma=False,
    )
```

```python
import jax
import jax.numpy as jnp
from jax import lax
from jax.experimental import pallas as pl
from jax.experimental.pallas import tpu as pltpu
from jax.sharding import Mesh
from jax.sharding import PartitionSpec as P

FS = ("z", "y")
TP = ("x", "c")

epsilon = 1e-06

LATE = 256
TAIL_VMEM = 20 * 2**20
FETCH_VMEM = 48 * 2**20
THEIRS_VMEM = 42 * 2**20


def early_kernel(normed_ref, own_ref, one_ref, two_ref, three_ref, scale_ref, out_ref, weight_ref):
    groups, members, rows, width = weight_ref.shape
    for d, block in enumerate((own_ref, one_ref, two_ref, three_ref)):
        member = lax.rem(lax.axis_index("y") + members - d, members)
        weight_ref[:, pl.ds(member, 1)] = block[...].reshape(groups, 1, rows, width)
    pre = jnp.dot(
        normed_ref[...],
        weight_ref[...].reshape(groups * members * rows, width),
        preferred_element_type=jnp.float32,
    )
    kept = jnp.maximum(pre * scale_ref[...], 0.0)
    out_ref[...] = (kept * kept).astype(out_ref.dtype)


def early_block(normed, blocks, scale):
    groups, rows, width = blocks[0].shape
    vmem = pl.BlockSpec(memory_space=pltpu.VMEM)
    tokens, features = normed.shape
    return pl.pallas_call(
        early_kernel,
        in_specs=[vmem] * (2 + len(blocks)),
        out_specs=vmem,
        out_shape=jax.ShapeDtypeStruct((tokens, width), jnp.bfloat16),
        scratch_shapes=[pltpu.VMEM((groups, len(blocks), rows, width), jnp.bfloat16)],
        cost_estimate=pl.CostEstimate(
            flops=2 * tokens * features * width,
            bytes_accessed=2 * (tokens * features + features * width + tokens * width),
            transcendentals=0,
        ),
        compiler_params=pltpu.CompilerParams(vmem_limit_bytes=20 * 2**20),
    )(normed, *blocks, scale.reshape(1, width))


def prepare_kernel(up_ref, down_ref, scale_ref, copies_ref, early_ref):
    rows, width = down_ref.shape
    early_width = early_ref.shape[1]
    late_width = width - early_width
    late_rows = copies_ref.shape[1] - rows
    at = lax.broadcasted_iota(jnp.int32, (rows, rows), 0)
    to = lax.broadcasted_iota(jnp.int32, (rows, rows), 1)
    scale = jnp.sum(jnp.where(at == to, scale_ref[...], 0.0), axis=1, keepdims=True)
    down = (down_ref[...] * scale).astype(jnp.bfloat16)
    early_ref[...] = up_ref[:, :early_width].astype(jnp.bfloat16)
    for k in range(copies_ref.shape[0]):
        copies_ref[k, :rows, :] = down
        for i in range(rows // late_rows):
            copies_ref[k, rows:, i * late_width : (i + 1) * late_width] = up_ref[
                i * late_rows : (i + 1) * late_rows, early_width:
            ].astype(jnp.bfloat16)


def products(early, late, weight):
    early_width = early.shape[1]
    contract = (((1,), (1,)), ((), ()))
    return lax.dot_general(
        early, weight[:, :early_width], contract, preferred_element_type=jnp.float32
    ) + lax.dot_general(
        late, weight[:, early_width:], contract, preferred_element_type=jnp.float32
    )


def side_weight(down_ref, side, i, blocks, columns):
    groups = down_ref.shape[0] // (2 * blocks)
    first = (2 * i + side) * groups
    weight = down_ref[pl.ds(first, groups)]
    return weight.reshape(columns, down_ref.shape[2])


def late_kernel(view_ref, late_ref, sem):
    late = pltpu.make_async_copy(view_ref.at[:, view_ref.shape[1] - 1], late_ref, sem)
    late.start()
    late.wait()


def late_weights(gathered, rows, width):
    places, all_rows, depth = gathered.shape
    late_rows = all_rows - rows
    parts = depth // width
    view = gathered.reshape(places, all_rows // late_rows, late_rows, parts, width)
    view = view.transpose(0, 1, 3, 2, 4)
    late = pl.pallas_call(
        late_kernel,
        in_specs=[pl.BlockSpec(memory_space=pltpu.HBM)],
        out_specs=pl.BlockSpec(memory_space=pltpu.VMEM),
        out_shape=jax.ShapeDtypeStruct((places, parts, late_rows, width), gathered.dtype),
        scratch_shapes=[pltpu.SemaphoreType.DMA],
        cost_estimate=pl.CostEstimate(
            flops=1000, bytes_accessed=4 * places * late_rows * depth, transcendentals=0
        ),
        compiler_params=pltpu.CompilerParams(vmem_limit_bytes=FETCH_VMEM),
    )(view)
    return late.reshape(-1, width)


def theirs_kernel(
    early_ref, normed_ref, weight_ref, scale_ref, gathered_ref, theirs_ref, late_ref, down_ref, sems
):
    blocks, _, columns = theirs_ref.shape
    rows = down_ref.shape[1]
    groups = columns // rows
    core = lax.axis_index("c")
    copies = []
    for n, side in enumerate((1 - core, core)):
        for i in range(blocks):
            part = pl.ds((2 * i + side) * groups, groups)
            copies.append(
                pltpu.make_async_copy(
                    gathered_ref.at[part, pl.ds(0, rows)], down_ref.at[part], sems.at[n * blocks + i]
                )
            )
    for copy in copies:
        copy.start()
    pre = jnp.dot(normed_ref[...], weight_ref[...], preferred_element_type=jnp.float32)
    kept = jnp.maximum(pre * scale_ref[...], 0.0)
    late_ref[...] = (kept * kept).astype(late_ref.dtype)
    for i in range(blocks):
        copies[i].wait()
        weight = side_weight(down_ref, 1 - core, i, blocks, columns)
        theirs_ref[i] = products(early_ref[...], late_ref[...], weight).astype(theirs_ref.dtype)
    for copy in copies[blocks:]:
        copy.wait()


def theirs_blocks(early, normed, late_weight, scale, gathered, rows, columns, blocks):
    tokens, features = normed.shape
    places, _, depth = gathered.shape
    width = scale.shape[0]
    vmem = pl.BlockSpec(memory_space=pltpu.VMEM)
    return pl.pallas_call(
        theirs_kernel,
        in_specs=[vmem] * 4 + [pl.BlockSpec(memory_space=pltpu.HBM)],
        out_specs=[vmem] * 3,
        out_shape=[
            jax.ShapeDtypeStruct((blocks, tokens, columns), jnp.bfloat16),
            jax.ShapeDtypeStruct((tokens, width), jnp.bfloat16),
            jax.ShapeDtypeStruct((places, rows, depth), jnp.bfloat16),
        ],
        scratch_shapes=[pltpu.SemaphoreType.DMA((2 * blocks,))],
        cost_estimate=pl.CostEstimate(
            flops=2 * tokens * (depth * columns * blocks + features * width),
            bytes_accessed=2 * (tokens * features + columns * depth * blocks),
            transcendentals=0,
        ),
        compiler_params=pltpu.CompilerParams(vmem_limit_bytes=THEIRS_VMEM),
    )(early, normed, late_weight, scale.reshape(1, width), gathered)


def mine_kernel(early_ref, late_ref, down_ref, out_ref):
    blocks, _, columns = out_ref.shape
    for i in range(blocks):
        weight = side_weight(down_ref, lax.axis_index("c"), i, blocks, columns)
        out_ref[i] = products(early_ref[...], late_ref[...], weight)


def mine_blocks(early, late, down, columns, blocks):
    tokens = early.shape[0]
    depth = down.shape[2]
    vmem = pl.BlockSpec(memory_space=pltpu.VMEM)
    return pl.pallas_call(
        mine_kernel,
        in_specs=[vmem] * 3,
        out_specs=vmem,
        out_shape=jax.ShapeDtypeStruct((blocks, tokens, columns), jnp.float32),
        cost_estimate=pl.CostEstimate(
            flops=2 * tokens * depth * columns * blocks,
            bytes_accessed=2 * (tokens * depth + columns * depth * blocks),
            transcendentals=0,
        ),
        compiler_params=pltpu.CompilerParams(vmem_limit_bytes=TAIL_VMEM),
    )(early, late, down)


def sum_kernel(tiles_ref, out_ref):
    total = tiles_ref[0].astype(jnp.float32)
    for i in range(1, tiles_ref.shape[0]):
        total = total + tiles_ref[i].astype(jnp.float32)
    out_ref[...] = total.astype(out_ref.dtype)


def local(tokens, norm_gain, up_weight, up_scale, down_weight, down_scale):
    rows, hidden_width = up_weight.shape
    early_width = hidden_width - LATE
    parts = hidden_width // LATE
    late_rows = rows // parts
    vmem = pl.BlockSpec(memory_space=pltpu.VMEM)
    copies, early = pl.pallas_call(
        prepare_kernel,
        in_specs=[vmem, vmem, vmem],
        out_specs=[vmem, vmem],
        out_shape=[
            jax.ShapeDtypeStruct(
                (lax.axis_size("y"), rows + late_rows, hidden_width), jnp.bfloat16
            ),
            jax.ShapeDtypeStruct((rows, early_width), jnp.bfloat16),
        ],
    )(up_weight, down_weight.T, down_scale.reshape(1, rows))
    both = lax.all_to_all(copies, "y", 0, 0, tiled=True)
    early, both = lax.optimization_barrier((early, both))
    gathered = lax.all_gather(both, "z", axis=0, tiled=True)
    early = lax.all_gather(early, "z", axis=0, tiled=False)
    early, tokens, up_scale = lax.optimization_barrier((early, tokens, up_scale))
    members = lax.axis_size("y")

    def sent(d):
        return lax.ppermute(early, "y", [(i, (i + d) % members) for i in range(members)])

    two, one, three = sent(2), sent(1), sent(3)

    floats = tokens.astype(jnp.float32)
    inverse = lax.rsqrt(jnp.mean(floats * floats, axis=-1, keepdims=True) + epsilon)
    normed = lax.optimization_barrier((floats * inverse * norm_gain).astype(jnp.bfloat16))

    early_hidden = early_block(
        normed, (early, one, two, three), up_scale[:early_width]
    )
    cores, chips = lax.axis_size("c"), lax.axis_size("x")
    columns = rows * lax.axis_size("z") * lax.axis_size("y") // (cores * chips)
    late_weight = late_weights(gathered, rows, LATE)
    theirs, late_hidden, down = theirs_blocks(
        early_hidden, normed, late_weight, up_scale[early_width:], gathered, rows, columns, chips
    )
    arrived = lax.ppermute(theirs, "c", [(0, 1), (1, 0)])
    mine = mine_blocks(early_hidden, late_hidden, down, columns, chips)
    chip_sum = (mine + arrived.astype(jnp.float32)).astype(jnp.bfloat16)
    tiles = lax.all_to_all(chip_sum, "x", 0, 0, tiled=True)
    return pl.pallas_call(
        sum_kernel,
        in_specs=[vmem],
        out_specs=vmem,
        out_shape=jax.ShapeDtypeStruct(tiles.shape[1:], tiles.dtype),
        compiler_params=pltpu.CompilerParams(vmem_limit_bytes=TAIL_VMEM),
    )(tiles)


def solution(mesh):
    split = Mesh(mesh.devices.reshape(16, 4, 4, 2), FS + TP)
    return jax.shard_map(
        local,
        mesh=split,
        in_specs=(P(FS, None), P(), P(FS, TP), P(TP), P(TP, FS), P(FS)),
        out_specs=P(FS, TP),
        check_vma=False,
    )
```

```python
import jax
import jax.numpy as jnp
from jax import lax
from jax.experimental import pallas as pl
from jax.experimental.pallas import tpu as pltpu
from jax.sharding import Mesh
from jax.sharding import PartitionSpec as P

FS = ("z", "y")
TP = ("x", "c")

epsilon = 1e-06

LATE = 256
TAIL_VMEM = 20 * 2**20
FETCH_VMEM = 48 * 2**20


def early_kernel(normed_ref, own_ref, one_ref, two_ref, three_ref, scale_ref, out_ref, weight_ref):
    groups, members, rows, width = weight_ref.shape
    for d, block in enumerate((own_ref, one_ref, two_ref, three_ref)):
        member = lax.rem(lax.axis_index("y") + members - d, members)
        weight_ref[:, pl.ds(member, 1)] = block[...].reshape(groups, 1, rows, width)
    pre = jnp.dot(
        normed_ref[...],
        weight_ref[...].reshape(groups * members * rows, width),
        preferred_element_type=jnp.float32,
    )
    kept = jnp.maximum(pre * scale_ref[...], 0.0)
    out_ref[...] = (kept * kept).astype(out_ref.dtype)


def early_block(normed, blocks, scale):
    groups, rows, width = blocks[0].shape
    vmem = pl.BlockSpec(memory_space=pltpu.VMEM)
    tokens, features = normed.shape
    return pl.pallas_call(
        early_kernel,
        in_specs=[vmem] * (2 + len(blocks)),
        out_specs=vmem,
        out_shape=jax.ShapeDtypeStruct((tokens, width), jnp.bfloat16),
        scratch_shapes=[pltpu.VMEM((groups, len(blocks), rows, width), jnp.bfloat16)],
        cost_estimate=pl.CostEstimate(
            flops=2 * tokens * features * width,
            bytes_accessed=2 * (tokens * features + features * width + tokens * width),
            transcendentals=0,
        ),
        compiler_params=pltpu.CompilerParams(vmem_limit_bytes=20 * 2**20),
    )(normed, *blocks, scale.reshape(1, width))


def prepare_kernel(up_ref, down_ref, scale_ref, copies_ref, early_ref):
    rows, width = down_ref.shape
    early_width = early_ref.shape[1]
    late_width = width - early_width
    late_rows = copies_ref.shape[1] - rows
    at = lax.broadcasted_iota(jnp.int32, (rows, rows), 0)
    to = lax.broadcasted_iota(jnp.int32, (rows, rows), 1)
    scale = jnp.sum(jnp.where(at == to, scale_ref[...], 0.0), axis=1, keepdims=True)
    down = (down_ref[...] * scale).astype(jnp.bfloat16)
    early_ref[...] = up_ref[:, :early_width].astype(jnp.bfloat16)
    for k in range(copies_ref.shape[0]):
        copies_ref[k, :rows, :] = down
        for i in range(rows // late_rows):
            copies_ref[k, rows:, i * late_width : (i + 1) * late_width] = up_ref[
                i * late_rows : (i + 1) * late_rows, early_width:
            ].astype(jnp.bfloat16)


def products(early, late, weight):
    early_width = early.shape[1]
    contract = (((1,), (1,)), ((), ()))
    return lax.dot_general(
        early, weight[:, :early_width], contract, preferred_element_type=jnp.float32
    ) + lax.dot_general(
        late, weight[:, early_width:], contract, preferred_element_type=jnp.float32
    )


def side_weight(down_ref, side, i, blocks, columns):
    groups = down_ref.shape[0] // (2 * blocks)
    first = (2 * i + side) * groups
    weight = down_ref[pl.ds(first, groups)]
    return weight.reshape(columns, down_ref.shape[2])


def fetch_kernel(gathered_ref, late_view_ref, down_ref, late_ref, sems):
    rows = down_ref.shape[1]
    late = pltpu.make_async_copy(
        late_view_ref.at[:, late_view_ref.shape[1] - 1], late_ref, sems.at[0]
    )
    down = pltpu.make_async_copy(gathered_ref.at[:, pl.ds(0, rows)], down_ref, sems.at[1])
    late.start()
    down.start()
    late.wait()
    down.wait()


def fetched(gathered, rows, width):
    places, all_rows, depth = gathered.shape
    late_rows = all_rows - rows
    parts = depth // width
    view = gathered.reshape(places, all_rows // late_rows, late_rows, parts, width)
    view = view.transpose(0, 1, 3, 2, 4)
    vmem = pl.BlockSpec(memory_space=pltpu.VMEM)
    hbm = pl.BlockSpec(memory_space=pltpu.HBM)
    down, late = pl.pallas_call(
        fetch_kernel,
        in_specs=[hbm, hbm],
        out_specs=[vmem, vmem],
        out_shape=[
            jax.ShapeDtypeStruct((places, rows, depth), gathered.dtype),
            jax.ShapeDtypeStruct((places, parts, late_rows, width), gathered.dtype),
        ],
        scratch_shapes=[pltpu.SemaphoreType.DMA((2,))],
        cost_estimate=pl.CostEstimate(
            flops=1000, bytes_accessed=4 * places * all_rows * depth, transcendentals=0
        ),
        compiler_params=pltpu.CompilerParams(vmem_limit_bytes=FETCH_VMEM),
    )(gathered, view)
    return down, late.reshape(-1, width)


def theirs_kernel(
    early_ref, normed_ref, weight_ref, scale_ref, down_ref, theirs_ref, late_ref
):
    blocks, _, columns = theirs_ref.shape
    pre = jnp.dot(normed_ref[...], weight_ref[...], preferred_element_type=jnp.float32)
    kept = jnp.maximum(pre * scale_ref[...], 0.0)
    late_ref[...] = (kept * kept).astype(late_ref.dtype)

    @pl.loop(0, blocks)
    def _(i):
        weight = side_weight(down_ref, 1 - lax.axis_index("c"), i, blocks, columns)
        theirs_ref[i] = products(early_ref[...], late_ref[...], weight).astype(theirs_ref.dtype)


def theirs_blocks(early, normed, late_weight, scale, down, columns, blocks):
    tokens, features = normed.shape
    depth = down.shape[2]
    width = scale.shape[0]
    vmem = pl.BlockSpec(memory_space=pltpu.VMEM)
    return pl.pallas_call(
        theirs_kernel,
        in_specs=[vmem] * 5,
        out_specs=[vmem] * 2,
        out_shape=[
            jax.ShapeDtypeStruct((blocks, tokens, columns), jnp.bfloat16),
            jax.ShapeDtypeStruct((tokens, width), jnp.bfloat16),
        ],
        cost_estimate=pl.CostEstimate(
            flops=2 * tokens * (depth * columns * blocks + features * width),
            bytes_accessed=2 * (tokens * features + columns * depth * blocks),
            transcendentals=0,
        ),
        compiler_params=pltpu.CompilerParams(vmem_limit_bytes=TAIL_VMEM),
    )(early, normed, late_weight, scale.reshape(1, width), down)


def mine_kernel(early_ref, late_ref, down_ref, out_ref):
    blocks, _, columns = out_ref.shape

    @pl.loop(0, blocks)
    def _(i):
        weight = side_weight(down_ref, lax.axis_index("c"), i, blocks, columns)
        out_ref[i] = products(early_ref[...], late_ref[...], weight)


def mine_blocks(early, late, down, columns, blocks):
    tokens = early.shape[0]
    depth = down.shape[2]
    vmem = pl.BlockSpec(memory_space=pltpu.VMEM)
    return pl.pallas_call(
        mine_kernel,
        in_specs=[vmem] * 3,
        out_specs=vmem,
        out_shape=jax.ShapeDtypeStruct((blocks, tokens, columns), jnp.float32),
        cost_estimate=pl.CostEstimate(
            flops=2 * tokens * depth * columns * blocks,
            bytes_accessed=2 * (tokens * depth + columns * depth * blocks),
            transcendentals=0,
        ),
        compiler_params=pltpu.CompilerParams(vmem_limit_bytes=TAIL_VMEM),
    )(early, late, down)


def sum_kernel(tiles_ref, out_ref):
    total = tiles_ref[0].astype(jnp.float32)
    for i in range(1, tiles_ref.shape[0]):
        total = total + tiles_ref[i].astype(jnp.float32)
    out_ref[...] = total.astype(out_ref.dtype)


def local(tokens, norm_gain, up_weight, up_scale, down_weight, down_scale):
    rows, hidden_width = up_weight.shape
    early_width = hidden_width - LATE
    parts = hidden_width // LATE
    late_rows = rows // parts
    vmem = pl.BlockSpec(memory_space=pltpu.VMEM)
    copies, early = pl.pallas_call(
        prepare_kernel,
        in_specs=[vmem, vmem, vmem],
        out_specs=[vmem, vmem],
        out_shape=[
            jax.ShapeDtypeStruct(
                (lax.axis_size("y"), rows + late_rows, hidden_width), jnp.bfloat16
            ),
            jax.ShapeDtypeStruct((rows, early_width), jnp.bfloat16),
        ],
    )(up_weight, down_weight.T, down_scale.reshape(1, rows))
    both = lax.all_to_all(copies, "y", 0, 0, tiled=True)
    early, both = lax.optimization_barrier((early, both))
    gathered = lax.all_gather(both, "z", axis=0, tiled=True)
    early = lax.all_gather(early, "z", axis=0, tiled=False)
    early, tokens, up_scale = lax.optimization_barrier((early, tokens, up_scale))
    members = lax.axis_size("y")

    def sent(d):
        return lax.ppermute(early, "y", [(i, (i + d) % members) for i in range(members)])

    two, one, three = sent(2), sent(1), sent(3)

    floats = tokens.astype(jnp.float32)
    inverse = lax.rsqrt(jnp.mean(floats * floats, axis=-1, keepdims=True) + epsilon)
    normed = lax.optimization_barrier((floats * inverse * norm_gain).astype(jnp.bfloat16))

    early_hidden = early_block(
        normed, (early, one, two, three), up_scale[:early_width]
    )
    cores, chips = lax.axis_size("c"), lax.axis_size("x")
    columns = rows * lax.axis_size("z") * lax.axis_size("y") // (cores * chips)
    down, late_weight = fetched(gathered, rows, LATE)
    theirs, late_hidden = theirs_blocks(
        early_hidden, normed, late_weight, up_scale[early_width:], down, columns, chips
    )
    arrived = lax.ppermute(theirs, "c", [(0, 1), (1, 0)])
    mine = mine_blocks(early_hidden, late_hidden, down, columns, chips)
    chip_sum = (mine + arrived.astype(jnp.float32)).astype(jnp.bfloat16)
    tiles = lax.all_to_all(chip_sum, "x", 0, 0, tiled=True)
    return pl.pallas_call(
        sum_kernel,
        in_specs=[vmem],
        out_specs=vmem,
        out_shape=jax.ShapeDtypeStruct(tiles.shape[1:], tiles.dtype),
        compiler_params=pltpu.CompilerParams(vmem_limit_bytes=TAIL_VMEM),
    )(tiles)


def solution(mesh):
    split = Mesh(mesh.devices.reshape(16, 4, 4, 2), FS + TP)
    return jax.shard_map(
        local,
        mesh=split,
        in_specs=(P(FS, None), P(), P(FS, TP), P(TP), P(TP, FS), P(FS)),
        out_specs=P(FS, TP),
        check_vma=False,
    )
```

```python
import jax
import jax.numpy as jnp
from jax import lax
from jax.experimental import pallas as pl
from jax.experimental.pallas import tpu as pltpu
from jax.sharding import Mesh
from jax.sharding import PartitionSpec as P

FS = ("z", "y")
TP = ("x", "c")

epsilon = 1e-06

LATE = 256
TAIL_VMEM = 20 * 2**20
FETCH_VMEM = 48 * 2**20


def early_kernel(normed_ref, own_ref, one_ref, two_ref, three_ref, scale_ref, out_ref, weight_ref):
    groups, members, rows, width = weight_ref.shape
    for d, block in enumerate((own_ref, one_ref, two_ref, three_ref)):
        member = lax.rem(lax.axis_index("y") + members - d, members)
        weight_ref[:, pl.ds(member, 1)] = block[...].reshape(groups, 1, rows, width)
    pre = jnp.dot(
        normed_ref[...],
        weight_ref[...].reshape(groups * members * rows, width),
        preferred_element_type=jnp.float32,
    )
    kept = jnp.maximum(pre * scale_ref[...], 0.0)
    out_ref[...] = (kept * kept).astype(out_ref.dtype)


def early_block(normed, blocks, scale):
    groups, rows, width = blocks[0].shape
    vmem = pl.BlockSpec(memory_space=pltpu.VMEM)
    tokens, features = normed.shape
    return pl.pallas_call(
        early_kernel,
        in_specs=[vmem] * (2 + len(blocks)),
        out_specs=vmem,
        out_shape=jax.ShapeDtypeStruct((tokens, width), jnp.bfloat16),
        scratch_shapes=[pltpu.VMEM((groups, len(blocks), rows, width), jnp.bfloat16)],
        cost_estimate=pl.CostEstimate(
            flops=2 * tokens * features * width,
            bytes_accessed=2 * (tokens * features + features * width + tokens * width),
            transcendentals=0,
        ),
        compiler_params=pltpu.CompilerParams(vmem_limit_bytes=20 * 2**20),
    )(normed, *blocks, scale.reshape(1, width))


def prepare_kernel(up_ref, down_ref, scale_ref, copies_ref, early_ref):
    rows, width = down_ref.shape
    early_width = early_ref.shape[1]
    late_width = width - early_width
    late_rows = copies_ref.shape[1] - rows
    at = lax.broadcasted_iota(jnp.int32, (rows, rows), 0)
    to = lax.broadcasted_iota(jnp.int32, (rows, rows), 1)
    scale = jnp.sum(jnp.where(at == to, scale_ref[...], 0.0), axis=1, keepdims=True)
    down = (down_ref[...] * scale).astype(jnp.bfloat16)
    early_ref[...] = up_ref[:, :early_width].astype(jnp.bfloat16)

    @pl.loop(0, copies_ref.shape[0])
    def _(k):
        copies_ref[k, :rows, :] = down
        for i in range(rows // late_rows):
            copies_ref[k, rows:, i * late_width : (i + 1) * late_width] = up_ref[
                i * late_rows : (i + 1) * late_rows, early_width:
            ].astype(jnp.bfloat16)


def products(early, late, weight):
    early_width = early.shape[1]
    contract = (((1,), (1,)), ((), ()))
    return lax.dot_general(
        early, weight[:, :early_width], contract, preferred_element_type=jnp.float32
    ) + lax.dot_general(
        late, weight[:, early_width:], contract, preferred_element_type=jnp.float32
    )


def side_weight(down_ref, side, i, blocks, columns):
    groups = down_ref.shape[0] // (2 * blocks)
    first = (2 * i + side) * groups
    weight = down_ref[pl.ds(first, groups)]
    return weight.reshape(columns, down_ref.shape[2])


def fetch_kernel(gathered_ref, late_view_ref, down_ref, late_ref, sems):
    rows = down_ref.shape[1]
    late = pltpu.make_async_copy(
        late_view_ref.at[:, late_view_ref.shape[1] - 1], late_ref, sems.at[0]
    )
    down = pltpu.make_async_copy(gathered_ref.at[:, pl.ds(0, rows)], down_ref, sems.at[1])
    late.start()
    down.start()
    late.wait()
    down.wait()


def fetched(gathered, rows, width):
    places, all_rows, depth = gathered.shape
    late_rows = all_rows - rows
    parts = depth // width
    view = gathered.reshape(places, all_rows // late_rows, late_rows, parts, width)
    view = view.transpose(0, 1, 3, 2, 4)
    vmem = pl.BlockSpec(memory_space=pltpu.VMEM)
    hbm = pl.BlockSpec(memory_space=pltpu.HBM)
    down, late = pl.pallas_call(
        fetch_kernel,
        in_specs=[hbm, hbm],
        out_specs=[vmem, vmem],
        out_shape=[
            jax.ShapeDtypeStruct((places, rows, depth), gathered.dtype),
            jax.ShapeDtypeStruct((places, parts, late_rows, width), gathered.dtype),
        ],
        scratch_shapes=[pltpu.SemaphoreType.DMA((2,))],
        cost_estimate=pl.CostEstimate(
            flops=1000, bytes_accessed=4 * places * all_rows * depth, transcendentals=0
        ),
        compiler_params=pltpu.CompilerParams(vmem_limit_bytes=FETCH_VMEM),
    )(gathered, view)
    return down, late.reshape(-1, width)


def theirs_kernel(
    early_ref, normed_ref, weight_ref, scale_ref, down_ref, theirs_ref, late_ref
):
    blocks, _, columns = theirs_ref.shape
    chunk = normed_ref.shape[0] // 3

    @pl.loop(0, 3)
    def _(m):
        part = pl.ds(pl.multiple_of(m * chunk, chunk), chunk)
        pre = jnp.dot(normed_ref[part, :], weight_ref[...], preferred_element_type=jnp.float32)
        kept = jnp.maximum(pre * scale_ref[...], 0.0)
        late_ref[part, :] = (kept * kept).astype(late_ref.dtype)

    @pl.loop(0, blocks)
    def _(i):
        weight = side_weight(down_ref, 1 - lax.axis_index("c"), i, blocks, columns)
        theirs_ref[i] = products(early_ref[...], late_ref[...], weight).astype(theirs_ref.dtype)


def theirs_blocks(early, normed, late_weight, scale, down, columns, blocks):
    tokens, features = normed.shape
    depth = down.shape[2]
    width = scale.shape[0]
    vmem = pl.BlockSpec(memory_space=pltpu.VMEM)
    return pl.pallas_call(
        theirs_kernel,
        in_specs=[vmem] * 5,
        out_specs=[vmem] * 2,
        out_shape=[
            jax.ShapeDtypeStruct((blocks, tokens, columns), jnp.bfloat16),
            jax.ShapeDtypeStruct((tokens, width), jnp.bfloat16),
        ],
        cost_estimate=pl.CostEstimate(
            flops=2 * tokens * (depth * columns * blocks + features * width),
            bytes_accessed=2 * (tokens * features + columns * depth * blocks),
            transcendentals=0,
        ),
        compiler_params=pltpu.CompilerParams(vmem_limit_bytes=TAIL_VMEM),
    )(early, normed, late_weight, scale.reshape(1, width), down)


def mine_kernel(early_ref, late_ref, down_ref, out_ref):
    blocks, _, columns = out_ref.shape

    @pl.loop(0, blocks)
    def _(i):
        weight = side_weight(down_ref, lax.axis_index("c"), i, blocks, columns)
        out_ref[i] = products(early_ref[...], late_ref[...], weight)


def mine_blocks(early, late, down, columns, blocks):
    tokens = early.shape[0]
    depth = down.shape[2]
    vmem = pl.BlockSpec(memory_space=pltpu.VMEM)
    return pl.pallas_call(
        mine_kernel,
        in_specs=[vmem] * 3,
        out_specs=vmem,
        out_shape=jax.ShapeDtypeStruct((blocks, tokens, columns), jnp.float32),
        cost_estimate=pl.CostEstimate(
            flops=2 * tokens * depth * columns * blocks,
            bytes_accessed=2 * (tokens * depth + columns * depth * blocks),
            transcendentals=0,
        ),
        compiler_params=pltpu.CompilerParams(vmem_limit_bytes=TAIL_VMEM),
    )(early, late, down)


def sum_kernel(tiles_ref, out_ref):
    total = tiles_ref[0].astype(jnp.float32)
    for i in range(1, tiles_ref.shape[0]):
        total = total + tiles_ref[i].astype(jnp.float32)
    out_ref[...] = total.astype(out_ref.dtype)


def local(tokens, norm_gain, up_weight, up_scale, down_weight, down_scale):
    rows, hidden_width = up_weight.shape
    early_width = hidden_width - LATE
    parts = hidden_width // LATE
    late_rows = rows // parts
    vmem = pl.BlockSpec(memory_space=pltpu.VMEM)
    copies, early = pl.pallas_call(
        prepare_kernel,
        in_specs=[vmem, vmem, vmem],
        out_specs=[vmem, vmem],
        out_shape=[
            jax.ShapeDtypeStruct(
                (lax.axis_size("y"), rows + late_rows, hidden_width), jnp.bfloat16
            ),
            jax.ShapeDtypeStruct((rows, early_width), jnp.bfloat16),
        ],
    )(up_weight, down_weight.T, down_scale.reshape(1, rows))
    both = lax.all_to_all(copies, "y", 0, 0, tiled=True)
    early, both = lax.optimization_barrier((early, both))
    gathered = lax.all_gather(both, "z", axis=0, tiled=True)
    early = lax.all_gather(early, "z", axis=0, tiled=False)
    early, tokens, up_scale = lax.optimization_barrier((early, tokens, up_scale))
    members = lax.axis_size("y")

    def sent(d):
        return lax.ppermute(early, "y", [(i, (i + d) % members) for i in range(members)])

    two, one, three = sent(2), sent(1), sent(3)

    floats = tokens.astype(jnp.float32)
    inverse = lax.rsqrt(jnp.mean(floats * floats, axis=-1, keepdims=True) + epsilon)
    normed = lax.optimization_barrier((floats * inverse * norm_gain).astype(jnp.bfloat16))

    early_hidden = early_block(
        normed, (early, one, two, three), up_scale[:early_width]
    )
    cores, chips = lax.axis_size("c"), lax.axis_size("x")
    columns = rows * lax.axis_size("z") * lax.axis_size("y") // (cores * chips)
    down, late_weight = fetched(gathered, rows, LATE)
    theirs, late_hidden = theirs_blocks(
        early_hidden, normed, late_weight, up_scale[early_width:], down, columns, chips
    )
    arrived = lax.ppermute(theirs, "c", [(0, 1), (1, 0)])
    mine = mine_blocks(early_hidden, late_hidden, down, columns, chips)
    chip_sum = (mine + arrived.astype(jnp.float32)).astype(jnp.bfloat16)
    tiles = lax.all_to_all(chip_sum, "x", 0, 0, tiled=True)
    return pl.pallas_call(
        sum_kernel,
        in_specs=[vmem],
        out_specs=vmem,
        out_shape=jax.ShapeDtypeStruct(tiles.shape[1:], tiles.dtype),
        compiler_params=pltpu.CompilerParams(vmem_limit_bytes=TAIL_VMEM),
    )(tiles)


def solution(mesh):
    split = Mesh(mesh.devices.reshape(16, 4, 4, 2), FS + TP)
    return jax.shard_map(
        local,
        mesh=split,
        in_specs=(P(FS, None), P(), P(FS, TP), P(TP), P(TP, FS), P(FS)),
        out_specs=P(FS, TP),
        check_vma=False,
    )
```

```python
import jax
import jax.numpy as jnp
from jax import lax
from jax.experimental import pallas as pl
from jax.experimental.pallas import tpu as pltpu
from jax.sharding import Mesh
from jax.sharding import PartitionSpec as P

FS = ("z", "y")
TP = ("x", "c")

epsilon = 1e-06

LATE = 256
TAIL_VMEM = 20 * 2**20
FETCH_VMEM = 48 * 2**20


def early_kernel(normed_ref, own_ref, one_ref, two_ref, three_ref, scale_ref, out_ref, weight_ref):
    groups, members, rows, width = weight_ref.shape
    for d, block in enumerate((own_ref, one_ref, two_ref, three_ref)):
        member = lax.rem(lax.axis_index("y") + members - d, members)
        weight_ref[:, pl.ds(member, 1)] = block[...].reshape(groups, 1, rows, width)
    pre = jnp.dot(
        normed_ref[...],
        weight_ref[...].reshape(groups * members * rows, width),
        preferred_element_type=jnp.float32,
    )
    kept = jnp.maximum(pre * scale_ref[...], 0.0)
    out_ref[...] = (kept * kept).astype(out_ref.dtype)


def early_block(normed, blocks, scale):
    groups, rows, width = blocks[0].shape
    vmem = pl.BlockSpec(memory_space=pltpu.VMEM)
    tokens, features = normed.shape
    return pl.pallas_call(
        early_kernel,
        in_specs=[vmem] * (2 + len(blocks)),
        out_specs=vmem,
        out_shape=jax.ShapeDtypeStruct((tokens, width), jnp.bfloat16),
        scratch_shapes=[pltpu.VMEM((groups, len(blocks), rows, width), jnp.bfloat16)],
        cost_estimate=pl.CostEstimate(
            flops=2 * tokens * features * width,
            bytes_accessed=2 * (tokens * features + features * width + tokens * width),
            transcendentals=0,
        ),
        compiler_params=pltpu.CompilerParams(vmem_limit_bytes=20 * 2**20),
    )(normed, *blocks, scale.reshape(1, width))


def prepare_kernel(up_ref, down_ref, scale_ref, copies_ref, early_ref):
    rows, width = down_ref.shape
    early_width = early_ref.shape[1]
    late_width = width - early_width
    late_rows = copies_ref.shape[1] - rows
    at = lax.broadcasted_iota(jnp.int32, (rows, rows), 0)
    to = lax.broadcasted_iota(jnp.int32, (rows, rows), 1)
    scale = jnp.sum(jnp.where(at == to, scale_ref[...], 0.0), axis=1, keepdims=True)
    down = (down_ref[...] * scale).astype(jnp.bfloat16)
    early_ref[...] = up_ref[:, :early_width].astype(jnp.bfloat16)
    for k in range(copies_ref.shape[0]):
        copies_ref[k, :rows, :] = down
        for i in range(rows // late_rows):
            copies_ref[k, rows:, i * late_width : (i + 1) * late_width] = up_ref[
                i * late_rows : (i + 1) * late_rows, early_width:
            ].astype(jnp.bfloat16)


def products(early, late, weight):
    early_width = early.shape[1]
    contract = (((1,), (1,)), ((), ()))
    return lax.dot_general(
        early, weight[:, :early_width], contract, preferred_element_type=jnp.float32
    ) + lax.dot_general(
        late, weight[:, early_width:], contract, preferred_element_type=jnp.float32
    )


def side_weight(down_ref, side, i, blocks, columns):
    groups = down_ref.shape[0] // (2 * blocks)
    first = (2 * i + side) * groups
    weight = down_ref[pl.ds(first, groups)]
    return weight.reshape(columns, down_ref.shape[2])


def fetch_kernel(gathered_ref, late_view_ref, down_ref, late_ref, sems):
    rows = down_ref.shape[1]
    late = pltpu.make_async_copy(
        late_view_ref.at[:, late_view_ref.shape[1] - 1], late_ref, sems.at[0]
    )
    part = down_ref.shape[0] // 8
    downs = [
        pltpu.make_async_copy(
            gathered_ref.at[pl.ds(i * part, part), pl.ds(0, rows)],
            down_ref.at[pl.ds(i * part, part)],
            sems.at[1 + i],
        )
        for i in range(8)
    ]
    for copy in [late] + downs:
        copy.start()
    for copy in [late] + downs:
        copy.wait()


def fetched(gathered, rows, width):
    places, all_rows, depth = gathered.shape
    late_rows = all_rows - rows
    parts = depth // width
    view = gathered.reshape(places, all_rows // late_rows, late_rows, parts, width)
    view = view.transpose(0, 1, 3, 2, 4)
    vmem = pl.BlockSpec(memory_space=pltpu.VMEM)
    hbm = pl.BlockSpec(memory_space=pltpu.HBM)
    down, late = pl.pallas_call(
        fetch_kernel,
        in_specs=[hbm, hbm],
        out_specs=[vmem, vmem],
        out_shape=[
            jax.ShapeDtypeStruct((places, rows, depth), gathered.dtype),
            jax.ShapeDtypeStruct((places, parts, late_rows, width), gathered.dtype),
        ],
        scratch_shapes=[pltpu.SemaphoreType.DMA((9,))],
        cost_estimate=pl.CostEstimate(
            flops=1000, bytes_accessed=4 * places * all_rows * depth, transcendentals=0
        ),
        compiler_params=pltpu.CompilerParams(vmem_limit_bytes=FETCH_VMEM),
    )(gathered, view)
    return down, late.reshape(-1, width)


def theirs_kernel(
    early_ref, normed_ref, weight_ref, scale_ref, down_ref, theirs_ref, late_ref
):
    blocks, _, columns = theirs_ref.shape
    pre = jnp.dot(normed_ref[...], weight_ref[...], preferred_element_type=jnp.float32)
    kept = jnp.maximum(pre * scale_ref[...], 0.0)
    late_ref[...] = (kept * kept).astype(late_ref.dtype)

    @pl.loop(0, blocks)
    def _(i):
        weight = side_weight(down_ref, 1 - lax.axis_index("c"), i, blocks, columns)
        theirs_ref[i] = products(early_ref[...], late_ref[...], weight).astype(theirs_ref.dtype)


def theirs_blocks(early, normed, late_weight, scale, down, columns, blocks):
    tokens, features = normed.shape
    depth = down.shape[2]
    width = scale.shape[0]
    vmem = pl.BlockSpec(memory_space=pltpu.VMEM)
    return pl.pallas_call(
        theirs_kernel,
        in_specs=[vmem] * 5,
        out_specs=[vmem] * 2,
        out_shape=[
            jax.ShapeDtypeStruct((blocks, tokens, columns), jnp.bfloat16),
            jax.ShapeDtypeStruct((tokens, width), jnp.bfloat16),
        ],
        cost_estimate=pl.CostEstimate(
            flops=2 * tokens * (depth * columns * blocks + features * width),
            bytes_accessed=2 * (tokens * features + columns * depth * blocks),
            transcendentals=0,
        ),
        compiler_params=pltpu.CompilerParams(vmem_limit_bytes=TAIL_VMEM),
    )(early, normed, late_weight, scale.reshape(1, width), down)


def mine_kernel(early_ref, late_ref, down_ref, out_ref):
    blocks, _, columns = out_ref.shape

    @pl.loop(0, blocks)
    def _(i):
        weight = side_weight(down_ref, lax.axis_index("c"), i, blocks, columns)
        out_ref[i] = products(early_ref[...], late_ref[...], weight)


def mine_blocks(early, late, down, columns, blocks):
    tokens = early.shape[0]
    depth = down.shape[2]
    vmem = pl.BlockSpec(memory_space=pltpu.VMEM)
    return pl.pallas_call(
        mine_kernel,
        in_specs=[vmem] * 3,
        out_specs=vmem,
        out_shape=jax.ShapeDtypeStruct((blocks, tokens, columns), jnp.float32),
        cost_estimate=pl.CostEstimate(
            flops=2 * tokens * depth * columns * blocks,
            bytes_accessed=2 * (tokens * depth + columns * depth * blocks),
            transcendentals=0,
        ),
        compiler_params=pltpu.CompilerParams(vmem_limit_bytes=TAIL_VMEM),
    )(early, late, down)


def sum_kernel(tiles_ref, out_ref):
    total = tiles_ref[0].astype(jnp.float32)
    for i in range(1, tiles_ref.shape[0]):
        total = total + tiles_ref[i].astype(jnp.float32)
    out_ref[...] = total.astype(out_ref.dtype)


def local(tokens, norm_gain, up_weight, up_scale, down_weight, down_scale):
    rows, hidden_width = up_weight.shape
    early_width = hidden_width - LATE
    parts = hidden_width // LATE
    late_rows = rows // parts
    vmem = pl.BlockSpec(memory_space=pltpu.VMEM)
    copies, early = pl.pallas_call(
        prepare_kernel,
        in_specs=[vmem, vmem, vmem],
        out_specs=[vmem, vmem],
        out_shape=[
            jax.ShapeDtypeStruct(
                (lax.axis_size("y"), rows + late_rows, hidden_width), jnp.bfloat16
            ),
            jax.ShapeDtypeStruct((rows, early_width), jnp.bfloat16),
        ],
    )(up_weight, down_weight.T, down_scale.reshape(1, rows))
    both = lax.all_to_all(copies, "y", 0, 0, tiled=True)
    early, both = lax.optimization_barrier((early, both))
    gathered = lax.all_gather(both, "z", axis=0, tiled=True)
    early = lax.all_gather(early, "z", axis=0, tiled=False)
    early, tokens, up_scale = lax.optimization_barrier((early, tokens, up_scale))
    members = lax.axis_size("y")

    def sent(d):
        return lax.ppermute(early, "y", [(i, (i + d) % members) for i in range(members)])

    two, one, three = sent(2), sent(1), sent(3)

    floats = tokens.astype(jnp.float32)
    inverse = lax.rsqrt(jnp.mean(floats * floats, axis=-1, keepdims=True) + epsilon)
    normed = lax.optimization_barrier((floats * inverse * norm_gain).astype(jnp.bfloat16))

    early_hidden = early_block(
        normed, (early, one, two, three), up_scale[:early_width]
    )
    cores, chips = lax.axis_size("c"), lax.axis_size("x")
    columns = rows * lax.axis_size("z") * lax.axis_size("y") // (cores * chips)
    down, late_weight = fetched(gathered, rows, LATE)
    theirs, late_hidden = theirs_blocks(
        early_hidden, normed, late_weight, up_scale[early_width:], down, columns, chips
    )
    arrived = lax.ppermute(theirs, "c", [(0, 1), (1, 0)])
    mine = mine_blocks(early_hidden, late_hidden, down, columns, chips)
    chip_sum = (mine + arrived.astype(jnp.float32)).astype(jnp.bfloat16)
    tiles = lax.all_to_all(chip_sum, "x", 0, 0, tiled=True)
    return pl.pallas_call(
        sum_kernel,
        in_specs=[vmem],
        out_specs=vmem,
        out_shape=jax.ShapeDtypeStruct(tiles.shape[1:], tiles.dtype),
        compiler_params=pltpu.CompilerParams(vmem_limit_bytes=TAIL_VMEM),
    )(tiles)


def solution(mesh):
    split = Mesh(mesh.devices.reshape(16, 4, 4, 2), FS + TP)
    return jax.shard_map(
        local,
        mesh=split,
        in_specs=(P(FS, None), P(), P(FS, TP), P(TP), P(TP, FS), P(FS)),
        out_specs=P(FS, TP),
        check_vma=False,
    )
```
